32 devices in a mesh: ep: 4 (over z), tp: 8 (over y, x, core).
Axes of the slice: x: 2, y: 2, z: 4, core: 2. Of those that a mesh axis runs over, the one named last changes fastest.
Arguments:
- tokens: bfloat16 [640, 2048], P('ep', 'tp'), may hold values from -6 to 6
- cotangent: bfloat16 [640, 2048], P('ep', 'tp'), may hold values from -6 to 6
- routes: int32 [640, 2], P('ep'), may hold values from 0 to 23, all different within a row; in each aligned block of 160 rows (0 to 159, 160 to 319, ...) at most 14 rows name the same one
- gate_weights: float32 [640, 2], P('ep'), may hold values from 0.2 to 2.5
- expert_gate: bfloat16 [24, 2048, 512], P('ep', 'tp'), may hold values from -0.125 to 0.125
- expert_up: bfloat16 [24, 2048, 512], P('ep', 'tp'), may hold values from -0.125 to 0.125
- expert_down: bfloat16 [24, 512, 2048], P('ep', None, 'tp'), may hold values from -0.25 to 0.25
- shared_gate: bfloat16 [2048, 576], P('tp'), may hold values from -0.125 to 0.125
- shared_up: bfloat16 [2048, 576], P('tp'), may hold values from -0.125 to 0.125
- shared_down: bfloat16 [576, 2048], P(None, 'tp'), may hold values from -0.25 to 0.25
Outputs:
- token_grad: bfloat16 [640, 2048], P('ep', 'tp')
- weight_grad: float32 [640, 2], P('ep')
- expert_gate_grad: float32 [24, 2048, 512], P('ep', 'tp')
- expert_up_grad: float32 [24, 2048, 512], P('ep', 'tp')
- expert_down_grad: float32 [24, 512, 2048], P('ep', None, 'tp')
- shared_gate_grad: float32 [2048, 576], P('tp', 'ep')
- shared_up_grad: float32 [2048, 576], P('tp', 'ep')
- shared_down_grad: float32 [576, 2048], P('ep', 'tp')
- gate_rows_sq: float32 [24, 2048], P('ep', 'tp')
- up_rows_sq: float32 [24, 2048], P('ep', 'tp')
- down_rows_sq: float32 [24, 512], P('ep')
- shared_gate_rows_sq: float32 [2048], P('tp')
- shared_up_rows_sq: float32 [2048], P('tp')
- shared_down_rows_sq: float32 [576], P('ep')
The draws below stay inside these ranges and needn't reach their ends.
Inputs may be any that keep to these rules, and one draw needn't show every extreme that they name: `routes`: each row names 2 different experts. Among the rows of one index of ep (aligned blocks of 160 rows) no expert is named more than 14 times, a bound that some block reaches.
All inputs are finite; a program needn't handle non-finite values.
Results may differ from the reference program's by a relative error of at most 0.0059.
Values may be sent and summed in bfloat16 or wider, within the bound.
A program may use at most 64 MiB of HBM per device.

```python
import math
import jax
import jax.numpy as jnp
import numpy as np
from jax import lax

D = 2048
FF = 512
SF = 576
TOP = 2
TOK_DEV = 160
EXPERTS = 24
CAP = 14
TOKENS = 640
N_EP = 4


def levels(key, shape, cuts, smallest, top_value):
    def one(axis_at, parts):
        heights = jax.random.uniform(jax.random.fold_in(jax.random.fold_in(key, 6), axis_at), (parts,), jnp.float32, smallest / len(cuts), top_value / len(cuts))
        return jnp.repeat(jnp.exp(heights), shape[axis_at] // parts).reshape((-1,) + (1,) * (len(shape) - axis_at - 1))

    loudness = one(*cuts[0])
    for cut in cuts[1:]:
        loudness = loudness * one(*cut)
    return loudness


def deal_out(stream_key, own, number, rows, number_of, top, bound, lean):
    order = jax.random.permutation(stream_key, number_of)
    packed, usual = load_shares(number_of, rows * top, bound, lean, True), load_shares(number_of, rows * top, bound, lean, False)
    places = jnp.arange(number_of)

    def named(sizes, rotation):
        used = int((sizes > 0).sum())
        fixed = max(1, used // 4)
        passed = fixed + (places - fixed + rotation * (used - fixed)) % max(1, number_of - fixed)
        return jnp.zeros((number_of,), jnp.int32).at[order[jnp.where(places < fixed, places, passed)]].set(jnp.asarray(sizes, jnp.int32))

    sizes = jnp.where(number % 4 == 0, named(packed, number // 4), named(usual, number - number // 4 - 1))
    mixed = jax.random.permutation(jax.random.fold_in(own, 3), number_of)
    source_of, receiver = mixed[0:number_of // 2 * 2:2], mixed[1:number_of // 2 * 2:2]
    room = jnp.minimum(sizes[source_of] - 1, bound - sizes[receiver]) // 2
    room = jnp.where((source_of == order[0]) | (receiver == order[0]) | (sizes[receiver] == 0), 0, jnp.maximum(room, 0))
    passed = jax.random.randint(jax.random.fold_in(own, 4), (number_of // 2,), 0, 1 << 20) % (room + 1)
    sizes = sizes.at[source_of].add(-passed).at[receiver].add(passed)
    labels = jnp.searchsorted(jnp.cumsum(sizes), jnp.arange(rows * top), side="right").astype(jnp.int32)
    listing = labels.reshape(top, rows).T
    listing = listing[jax.random.permutation(jax.random.fold_in(own, 1), rows)]
    rotation = jax.random.randint(jax.random.fold_in(own, 2), (rows, 1), 0, top)
    return jnp.take_along_axis(listing, (jnp.arange(top)[None, :] + rotation) % top, axis=1)


def load_shares(count, total, limit, skew, full):
    portions = [(1 << 20) // math.isqrt(grade ** skew) + 1 for grade in range(1, count + 1)]
    largest = limit if full else min(limit, max(-(-total // count), total * portions[0] // sum(portions)))
    least = 1 if total - largest >= count - 1 else 0
    holding, rest = [largest] + [least] * (count - 1), total - largest - least * (count - 1)
    while rest > 0:
        movable = [i for i in range(1, count) if holding[i] < largest] or [i for i in range(1, count) if holding[i] < limit]
        mass, left = sum([portions[i] for i in movable]), rest
        for i in movable:
            more = min(limit - holding[i], max(1, left * portions[i] // mass), rest)
            holding[i] = holding[i] + more
            rest = rest - more
    return np.array(holding)


def noise(rng, dims, spread, bound, split=(), held_as=jnp.bfloat16):
    entries = spread * jax.random.normal(rng, dims, jnp.float32)
    if split:
        entries = entries * levels(rng, dims, split, -0.22, 0.18)
    return jnp.clip(entries, -bound, bound).astype(held_as)


def setup_inputs(seed: int = 0) -> dict:
    seeds = jax.random.split(jax.random.key(seed), 11)
    tokens = noise(seeds[0], (TOKENS, D), 1.0, 6.0, ((0, 4), (1, 8)))
    cotangent = noise(seeds[1], (TOKENS, D), 1.0, 6.0, ((0, 4), (1, 8)))
    routes_keys = jax.random.split(jax.random.fold_in(seeds[2], 1), TOKENS // TOK_DEV)
    routes_turns = jax.random.permutation(jax.random.fold_in(seeds[2], 3), TOKENS // TOK_DEV)
    routes = jax.vmap(lambda own, number: deal_out(jax.random.fold_in(seeds[2], 2), own, number, TOK_DEV, EXPERTS, TOP, CAP, 1))(routes_keys, routes_turns).reshape((TOKENS, TOP))
    gate_weights = jnp.clip(jnp.exp(math.log(2.5) - 2.5257286 * jax.random.uniform(seeds[3], (TOKENS, TOP), jnp.float32) ** levels(seeds[3], (TOKENS, TOP), ((0, 4),), -0.2, 0.2)), 0.2, 2.5)
    expert_gate = noise(seeds[4], (EXPERTS, D, FF), D ** -0.5, 0.125, ((0, 4), (1, 8)))
    expert_up = noise(seeds[5], (EXPERTS, D, FF), D ** -0.5, 0.125, ((0, 4), (1, 8)))
    expert_down = noise(seeds[6], (EXPERTS, FF, D), FF ** -0.5, 0.25, ((0, 4), (2, 8)))
    shared_gate = noise(seeds[7], (D, SF), D ** -0.5, 0.125, ((0, 8),))
    shared_up = noise(seeds[8], (D, SF), D ** -0.5, 0.125, ((0, 8),))
    shared_down = noise(seeds[9], (SF, D), SF ** -0.5, 0.25, ((1, 8),))
    return {"tokens": tokens, "cotangent": cotangent, "routes": routes, "gate_weights": gate_weights, "expert_gate": expert_gate, "expert_up": expert_up, "expert_down": expert_down, "shared_gate": shared_gate, "shared_up": shared_up, "shared_down": shared_down}


def silu_parts(pre):
    logistic = jax.nn.sigmoid(pre)
    return pre * logistic, logistic * (1.0 + pre * (1.0 - logistic))


def contract(left, right, left_dim, right_dim):
    return lax.dot_general(left, right, (((left_dim,), (right_dim,)), ((), ())), preferred_element_type=jnp.float32)


def reference(tokens, cotangent, routes, gate_weights, expert_gate, expert_up, expert_down, shared_gate, shared_up, shared_down):
    assigned = TOK_DEV * TOP
    owners = routes.reshape(N_EP, assigned).astype(jnp.int32)
    picked = (owners[:, :, None] == jnp.arange(EXPERTS, dtype=jnp.int32)[None, None, :]).astype(jnp.int32)
    slot_rank = jnp.sum((jnp.cumsum(picked, axis=1) - picked) * picked, axis=2).astype(jnp.int32)
    block_ids = jnp.arange(N_EP, dtype=jnp.int32)[:, None]
    global_tok = block_ids * TOK_DEV + (jnp.arange(assigned, dtype=jnp.int32) // TOP)[None, :]
    row_index = block_ids * CAP + slot_rank
    table = jnp.full((EXPERTS, N_EP * CAP), TOKENS, jnp.int32).at[owners, row_index].set(global_tok)
    weight_table = jnp.zeros((EXPERTS, N_EP * CAP), jnp.float32).at[owners, row_index].set(gate_weights.reshape(N_EP, assigned))
    zero_row = jnp.zeros((1, D), jnp.bfloat16)
    padded_tok = jnp.concatenate([tokens, zero_row], axis=0)
    padded_cot = jnp.concatenate([cotangent, zero_row], axis=0)

    def one_expert(inputs):
        chosen, weights, w_gate, w_up, w_down = inputs
        rows_x = padded_tok[chosen]
        rows_dy = padded_cot[chosen]
        gate_pre = jnp.dot(rows_x, w_gate, preferred_element_type=jnp.float32)
        up_pre = jnp.dot(rows_x, w_up, preferred_element_type=jnp.float32)
        back = contract(rows_dy, w_down, 1, 1)
        silu_out, silu_slope = silu_parts(gate_pre)
        hidden = (silu_out * up_pre).astype(jnp.bfloat16)
        dhidden = weights[:, None] * back
        grad_gate = (dhidden * up_pre * silu_slope).astype(jnp.bfloat16)
        grad_up = (dhidden * silu_out).astype(jnp.bfloat16)
        weighted = (weights[:, None] * rows_dy.astype(jnp.float32)).astype(jnp.bfloat16)
        gate_grad = jnp.sum(hidden.astype(jnp.float32) * back, axis=1)
        down_grad = contract(hidden, weighted, 0, 0)
        gate_wgrad = contract(rows_x, grad_gate, 0, 0)
        up_wgrad = contract(rows_x, grad_up, 0, 0)
        row_grad = contract(grad_gate, w_gate, 1, 1) + contract(grad_up, w_up, 1, 1)
        return gate_wgrad, up_wgrad, down_grad, row_grad.astype(jnp.bfloat16), gate_grad

    gate_wgrads, up_wgrads, down_grads, row_grads, gate_grads = lax.map(
        one_expert, (table, weight_table, expert_gate, expert_up, expert_down))
    routed = row_grads[owners, row_index].astype(jnp.float32).reshape(TOKENS, TOP, D).sum(axis=1)
    weight_grad = gate_grads[owners, row_index].reshape(TOKENS, TOP)

    s_gate = jnp.dot(tokens, shared_gate, preferred_element_type=jnp.float32)
    s_up = jnp.dot(tokens, shared_up, preferred_element_type=jnp.float32)
    s_back = contract(cotangent, shared_down, 1, 1)
    s_out, s_slope = silu_parts(s_gate)
    s_hidden = (s_out * s_up).astype(jnp.bfloat16)
    s_dgate = (s_back * s_up * s_slope).astype(jnp.bfloat16)
    s_dup = (s_back * s_out).astype(jnp.bfloat16)
    shared_gate_grad = contract(tokens, s_dgate, 0, 0)
    shared_up_grad = contract(tokens, s_dup, 0, 0)
    shared_down_grad = contract(s_hidden, cotangent, 0, 0)
    shared_rows = contract(s_dgate, shared_gate, 1, 1) + contract(s_dup, shared_up, 1, 1)
    token_grad = (routed + shared_rows).astype(jnp.bfloat16)
    return (token_grad, weight_grad, gate_wgrads, up_wgrads, down_grads,
            shared_gate_grad, shared_up_grad, shared_down_grad,
            jnp.sum(gate_wgrads * gate_wgrads, axis=2), jnp.sum(up_wgrads * up_wgrads, axis=2),
            jnp.sum(down_grads * down_grads, axis=2),
            jnp.sum(shared_gate_grad * shared_gate_grad, axis=1),
            jnp.sum(shared_up_grad * shared_up_grad, axis=1),
            jnp.sum(shared_down_grad * shared_down_grad, axis=1))
```

```python
import functools

import jax
import jax.numpy as jnp
from jax import lax
from jax.experimental import pallas as pl
from jax.experimental.pallas import tpu as pltpu
from jax.sharding import PartitionSpec as P

BF = jnp.bfloat16
F32 = jnp.float32
MESH = pl.DeviceIdType.MESH
VMEM = pl.BlockSpec(memory_space=pltpu.VMEM)
HBM = pl.BlockSpec(memory_space=pltpu.HBM)
LANES = 128
WAVE_ROWS = 16
VMEM_BYTES = 67_043_328
ROOM = 14 * 2**20


def up_to(value, unit):
    return (value + unit - 1) // unit * unit


def silu_parts(pre):
    logistic = jax.nn.sigmoid(pre)
    return (pre * logistic, logistic * (1.0 + pre * (1.0 - logistic)))


def remote(src, dst, send, recv, where):
    return pltpu.make_async_remote_copy(
        src_ref=src,
        dst_ref=dst,
        send_sem=send,
        recv_sem=recv,
        device_id=where,
        device_id_type=MESH,
    )


def dot(left, right, left_dim, right_dim, precision=None):
    return lax.dot_general(
        left,
        right,
        (((left_dim,), (right_dim,)), ((), ())),
        precision=precision,
        preferred_element_type=F32,
    )


def row_squares(square):
    ones = jnp.ones((8, square.shape[1]), BF)
    high = square.astype(BF)
    low = (square - high.astype(F32)).astype(BF)
    return (dot(ones, high, 1, 1) + dot(ones, low, 1, 1))[:1, :]


def join(parts, axis):
    return parts[0] if len(parts) == 1 else jnp.concatenate(parts, axis=axis)


def nearest(ep, n_ep, k):
    if k == 0:
        return ep
    left, right = ep, n_ep - 1 - ep
    both = jnp.minimum(left, right)
    paired = jnp.where(2 * both >= k, 1, 0)
    far = jnp.where(paired == 1, (k + 1) // 2, k - both)
    go_left = jnp.where(paired == 1, k % 2, jnp.where(left > right, 1, 0))
    return ep + far * (1 - 2 * go_left)


class Plan:
    def __init__(self, n_ep, n_tp, tok, picks, narrow, experts, ff, shared):
        self.n_ep, self.n_tp, self.tok, self.picks = n_ep, n_tp, tok, picks
        self.narrow, self.experts, self.ff = narrow, experts, ff
        all_experts = experts * n_ep
        self.capacity = max(2, (tok * picks + all_experts - 1) // all_experts)
        self.half = n_tp // 2
        self.nc = ff // LANES
        self.nr = self.half // self.nc
        self.bpw = max(
            b for b in range(1, n_ep + 1)
            if n_ep % b == 0 and (b == 1 or b * self.capacity <= WAVE_ROWS)
        )
        self.waves = n_ep // self.bpw
        self.slots = up_to(self.capacity * self.bpw, 16)
        self.rows = up_to(experts * self.slots, self.slots * 2 * self.nr)
        self.rc = self.rows // (2 * self.nr)
        self.wave_tok = self.bpw * tok
        self.sc = self.wave_tok // (2 * self.nr)
        self.cols = shared // n_ep
        self.cpc = -(-self.cols // self.nc)
        self.slab = 3 * self.rc + self.sc
        self.out_slab = self.slab + 16
        self.e_rows = up_to(experts, 8)
        assert self.half % self.nc == 0 and self.nr > 0 and self.rc <= LANES
        assert self.sc % 16 == 0 and 3 * self.cpc <= LANES

    def place(self, q, c):
        return (q // self.nr) * self.half + (q % self.nr) * self.nc + c

    def strip(self, index):
        row = index * self.slots
        return row // self.rc, row % self.rc


def main_kernel(
    p,
    x, dy, routes, weights, w_gate, w_up, w_down, sg_w, su_w, sd_w,
    token_out, weight_out, gate_out, up_out, down_out, sg_out, su_out, sd_out,
    gate_sq, up_sq, down_sq, sg_sq, su_sq, sd_sq,
    wg, wu, wd, sgv, suv, sdv, rts, gws, all_x, all_dy, all_meta,
    s_in, s_back, s_out_w, oh, recv_x, weighted, rw,
    full, got, held, landed, acts, pair, part, part_in, own, wpart, wpart_in,
    ts, ts_in, es, es_in,
    ld, zo, zs, zr, a_s, a_r, b_s, b_r, c_s, c_r, d_s, d_r, r_s, r_r, e_s, e_r, t_s, t_r,
):
    n_ep, n_tp, half, nc, nr = p.n_ep, p.n_tp, p.half, p.nc, p.nr
    ep, me = lax.axis_index("ep"), lax.axis_index("tp")
    parity = lax.rem(me, 2)
    mine = me // 2
    partner = {"tp": me + 1 - 2 * parity}
    others = [lax.rem(mine + d, half) for d in range(1, half)]
    places = [{"tp": 2 * j + parity} for j in others]
    eps = [lax.rem(ep + d, n_ep) for d in range(1, n_ep)]
    tps = [lax.rem(me + d, n_tp) for d in range(1, n_tp)]
    order = [nearest(ep, n_ep, k) for k in range(n_ep)]
    place = parity * half + mine

    barrier = pltpu.get_barrier_semaphore()
    for where in [{"ep": q} for q in eps] + [{"tp": q} for q in tps]:
        pl.semaphore_signal(barrier, inc=1, device_id=where, device_id_type=MESH)

    span = pl.ds(pl.multiple_of(ep * p.cols, 8), p.cols)
    sources = (
        (x, all_x.at[ep]), (dy, all_dy.at[ep]), (routes, rts), (weights, gws),
        (sg_w.at[span], sgv), (su_w.at[span], suv), (sd_w.at[span], sdv),
        (w_gate, wg), (w_up, wu), (w_down, wd),
    )
    loads = []
    for k, (src, dst) in enumerate(sources):
        loads.append(pltpu.make_async_copy(src, dst, ld.at[k]))
        loads[-1].start()

    loads[2].wait()
    loads[3].wait()
    all_meta[ep] = jnp.concatenate(
        [rts[...].astype(F32), gws[...]]
        + [jnp.zeros((all_meta.shape[1] - 2 * p.picks, p.tok), F32)] * (
            all_meta.shape[1] > 2 * p.picks
        ),
        axis=0,
    )
    loads[0].wait()
    loads[1].wait()
    pl.semaphore_wait(barrier, n_ep + n_tp - 2)

    blocks = (all_meta, all_x, all_dy)

    def relay(b, k, send, step):
        return remote(
            blocks[k].at[b], blocks[k].at[b], send, zr.at[b, k], {"ep": ep + step}
        )

    go_right, go_left = ep < n_ep - 1, ep > 0
    for cond, side, step in ((go_right, 0, 1), (go_left, 1, -1)):

        @pl.when(cond)
        def _(side=side, step=step):
            for k in range(3):
                relay(ep, k, zo.at[side, k], step).start()

    def arrive(k):
        b = order[k]
        if k == 0:
            return
        for a in range(3):
            relay(b, a, zs.at[b, a], 0).wait_recv()

            @pl.when((b < ep) & go_right)
            def _():
                relay(b, a, zs.at[b, a], 1).start()

            @pl.when((b > ep) & go_left)
            def _():
                relay(b, a, zs.at[b, a], -1).start()

    lane_n = lax.broadcasted_iota(jnp.int32, (p.cols, nc * LANES), 1)
    row_i = lax.broadcasted_iota(jnp.int32, (p.cols, nc * LANES), 0)
    chunk = lax.shift_right_logical(lane_n, 7)
    lane = lane_n - chunk * LANES

    def spread_map(k):
        inside = (lane >= k * p.cpc) & (lane < (k + 1) * p.cpc)
        same = row_i == chunk * p.cpc + lane - k * p.cpc
        return jnp.where(inside & same, 1.0, 0.0).astype(BF)

    for k in range(4, 7):
        loads[k].wait()
    maps = [spread_map(k) for k in range(3)]
    s_in[...] = (dot(sgv[...], maps[0], 0, 0) + dot(suv[...], maps[1], 0, 0)).astype(BF)
    s_back[...] = dot(sdv[...], maps[2], 0, 0).astype(BF)
    s_out_w[...] = (dot(maps[1], sgv[...], 0, 0) + dot(maps[2], suv[...], 0, 0)).astype(BF)

    ids = (
        ep * p.experts + lax.broadcasted_iota(jnp.int32, (p.e_rows, p.tok), 0)
    ).astype(F32)
    before = jnp.where(
        lax.broadcasted_iota(jnp.int32, (p.tok, p.tok), 0)
        < lax.broadcasted_iota(jnp.int32, (p.tok, p.tok), 1),
        1.0,
        0.0,
    ).astype(BF)
    place_in = lax.broadcasted_iota(jnp.int32, (p.slots, p.tok), 0).astype(F32)
    spare = p.rows - p.experts * p.slots

    def route(w):
        sums = [jnp.zeros((p.slots, 1), F32) for _ in range(p.experts)]
        for i in range(p.bpw):
            info = all_meta[order[w * p.bpw + i]]
            chosen = jnp.zeros((p.e_rows, p.tok), F32)
            weight_of = jnp.zeros((p.e_rows, p.tok), F32)
            for k in range(p.picks):
                same = info[k : k + 1, :] == ids
                chosen = jnp.where(same, 1.0, chosen)
                weight_of = jnp.where(
                    same, info[p.picks + k : p.picks + k + 1, :], weight_of
                )
            rank = dot(chosen.astype(BF), before, 1, 0)
            slot = jnp.where(chosen > 0.0, rank + float(p.capacity * i), -1.0)
            for e in range(p.experts):
                hot = place_in == slot[e : e + 1, :]
                oh[w, i, pl.ds(e * p.slots, p.slots), :] = jnp.where(hot, 1.0, 0.0).astype(BF)
                sums[e] = sums[e] + jnp.sum(
                    jnp.where(hot, weight_of[e : e + 1, :], 0.0), axis=1, keepdims=True
                )
            if spare:
                oh[w, i, pl.ds(p.experts * p.slots, spare), :] = jnp.zeros((spare, p.tok), BF)
        for e in range(p.experts):
            rw[w, pl.ds(e * p.slots, p.slots), :] = jnp.broadcast_to(sums[e], (p.slots, LANES))
        if spare:
            rw[w, pl.ds(p.experts * p.slots, spare), :] = jnp.zeros((spare, LANES), F32)

    def pick(w, source):
        total = dot(oh[w, 0], source[order[w * p.bpw]], 1, 0)
        for i in range(1, p.bpw):
            total = total + dot(oh[w, i], source[order[w * p.bpw + i]], 1, 0)
        return total

    def wave_rows(w, source):
        return join([source[order[w * p.bpw + i]] for i in range(p.bpw)], 0)

    def swap_copy(w):
        return remote(full.at[w, 1 - parity], got.at[w], a_s.at[w], a_r.at[w], partner)

    def put(w, e, kind, value):
        q, at = p.strip(e)
        for c in range(nc):
            full[
                w, q // nr, (q % nr) * nc + c, pl.ds(kind * p.rc + at, p.slots), :
            ] = value[:, c * LANES : (c + 1) * LANES]

    def fill(w):
        for i in range(p.bpw):
            arrive(w * p.bpw + i)
        route(w)
        recv_x[w] = pick(w, all_x).astype(BF)
        if w == 0:
            loads[7].wait()
            loads[8].wait()
        for kind, weight in ((0, wg), (1, wu)):
            for e in range(p.experts):
                put(w, e, kind, dot(recv_x[w, pl.ds(e * p.slots, p.slots), :], weight[e], 1, 0))
        recv_dy = pick(w, all_dy)
        weighted[w] = (rw[w][:, :1] * recv_dy).astype(BF)
        narrow_dy = recv_dy.astype(BF)
        if w == 0:
            loads[9].wait()
        for e in range(p.experts):
            put(w, e, 2, dot(narrow_dy[e * p.slots : (e + 1) * p.slots, :], wd[e], 1, 1))
        for s in range(p.experts, p.rows // p.slots):
            for kind in range(3):
                put(w, s, kind, jnp.zeros((p.slots, p.ff), F32))
        s = dot(wave_rows(w, all_x), s_in[...], 1, 0) + dot(
            wave_rows(w, all_dy), s_back[...], 1, 0
        )
        for q in range(2 * nr):
            for c in range(nc):
                full[w, q // nr, (q % nr) * nc + c, pl.ds(3 * p.rc, p.sc), :] = s[
                    q * p.sc : (q + 1) * p.sc, c * LANES : (c + 1) * LANES
                ]
        swap_copy(w).start()

    def scatter_copy(w, d):
        return remote(
            held.at[w, others[d]], landed.at[w, d], b_s.at[w, d], b_r.at[w, d], places[d]
        )

    def scatter(w):
        swap_copy(w).wait_recv()
        for d, j in enumerate(others):
            held[w, j] = (full[w, parity, j] + got[w, j]).astype(BF)
            scatter_copy(w, d).start()

    def gather_copy(w, d, block):
        ref = acts.at[w, block]
        return remote(ref, ref, c_s.at[w, d], c_r.at[w, d], places[d])

    def side_copy(w, d, block):
        ref = acts.at[w, block]
        return remote(ref, ref, d_s.at[w, d], d_r.at[w, d], partner)

    def activate(w):
        out = full[w, parity, mine] + got[w, mine]
        for d in range(half - 1):
            scatter_copy(w, d).wait_recv()
            out = out + landed[w, d].astype(F32)
        gate, up, back = (out[k * p.rc : (k + 1) * p.rc] for k in range(3))
        silu_out, silu_slope = silu_parts(gate)
        hidden = (silu_out * up).astype(BF)
        band = parity * nr + mine // nc
        weight = rw[w, pl.ds(pl.multiple_of(band * p.rc, p.rc), p.rc), :]
        dhidden = weight * back
        acts[w, place, pl.ds(0, p.rc), :] = hidden
        acts[w, place, pl.ds(p.rc, p.rc), :] = (dhidden * up * silu_slope).astype(BF)
        acts[w, place, pl.ds(2 * p.rc, p.rc), :] = (dhidden * silu_out).astype(BF)
        dots = dot(
            jnp.ones((16, LANES), F32), hidden.astype(F32) * back, 1, 1, lax.Precision.HIGHEST
        )
        high = dots.astype(BF).astype(F32)
        mid = (dots - high).astype(BF).astype(F32)
        low = dots - high - mid
        line = lax.broadcasted_iota(jnp.int32, dots.shape, 0)
        pieces = jnp.where(line == 0, high, jnp.where(line == 1, mid, low))
        acts[w, place, pl.ds(3 * p.rc, 16), pl.ds(0, p.rc)] = pieces.astype(BF)
        both = out[3 * p.rc :]
        at = lax.broadcasted_iota(jnp.int32, both.shape, 1)
        s_up = pltpu.roll(both, LANES - p.cpc, 1)
        s_bk = pltpu.roll(both, LANES - 2 * p.cpc, 1)
        s_out, s_slope = silu_parts(both)
        s_dgate = pltpu.roll(s_bk * s_up * s_slope, p.cpc, 1)
        s_dup = pltpu.roll(s_bk * s_out, 2 * p.cpc, 1)
        value = jnp.where(
            at < p.cpc,
            s_out * s_up,
            jnp.where(at < 2 * p.cpc, s_dgate, jnp.where(at < 3 * p.cpc, s_dup, 0.0)),
        )
        acts[w, place, pl.ds(3 * p.rc + 16, p.sc), :] = value.astype(BF)
        for d in range(half - 1):
            gather_copy(w, d, place).start()
        side_copy(w, 0, place).start()

    def origin(d):
        return lax.rem(mine + half - 1 - d, half)

    def forward(w):
        for d in range(half - 1):
            block = parity * half + origin(d)
            gather_copy(w, d, block).wait_recv()
            side_copy(w, 1 + d, block).start()

    def strip_of(w, kind, e):
        q, at = p.strip(e)
        return join(
            [acts[w, p.place(q, c), pl.ds(kind * p.rc + at, p.slots), :] for c in range(nc)], 1
        )

    def shared_rows(w):
        return join(
            [
                join(
                    [
                        acts[w, p.place(q, c), pl.ds(3 * p.rc + 16, p.sc), :]
                        for c in range(nc)
                    ],
                    1,
                )
                for q in range(2 * nr)
            ],
            0,
        )

    def home_copies(b):
        return (
            remote(part.at[b], part_in.at[ep], r_s.at[b, 0], r_r.at[ep, 0], {"ep": b}),
            remote(wpart.at[b], wpart_in.at[ep], r_s.at[b, 1], r_r.at[ep, 1], {"ep": b}),
        )

    def send_home(w):
        side_copy(w, 0, (1 - parity) * half + mine).wait_recv()
        for d in range(half - 1):
            side_copy(w, 1 + d, (1 - parity) * half + origin(d)).wait_recv()
        row_grad = []
        for e in range(p.experts):
            row_grad.append(
                (
                    dot(strip_of(w, 1, e), wg[e], 1, 1) + dot(strip_of(w, 2, e), wu[e], 1, 1)
                ).astype(BF)
            )
        if spare:
            row_grad.append(jnp.zeros((spare, p.narrow), BF))
        row_grad = join(row_grad, 0)
        s_grad = dot(shared_rows(w), s_out_w[...], 1, 0)
        row_e = lax.broadcasted_iota(jnp.int32, (p.e_rows, p.rc), 0)
        row_l = lax.broadcasted_iota(jnp.int32, (p.e_rows, p.rc), 1)
        masked = []
        for q in range(2 * nr):
            line = jnp.zeros((1, p.rc), F32)
            for c in range(nc):
                pieces = acts[w, p.place(q, c), pl.ds(3 * p.rc, 16), pl.ds(0, p.rc)].astype(F32)
                line = line + (pieces[0:1] + pieces[1:2] + pieces[2:3])
            row = row_l + q * p.rc
            inside = (row >= row_e * p.slots) & (row < (row_e + 1) * p.slots)
            masked.append(jnp.where(inside, line, 0.0))
        for i in range(p.bpw):
            b = order[w * p.bpw + i]
            value = dot(oh[w, i], row_grad, 0, 0) + s_grad[i * p.tok : (i + 1) * p.tok, :]

            info = all_meta[b]
            dot_of = jnp.zeros((p.e_rows, p.tok), F32)
            for q in range(2 * nr):
                dot_of = dot_of + dot(
                    masked[q], oh[w, i, pl.ds(q * p.rc, p.rc), :].astype(F32), 1, 0,
                    lax.Precision.HIGHEST,
                )
            for k in range(p.picks):
                wpart[b, pl.ds(k, 1), :] = jnp.sum(
                    jnp.where(info[k : k + 1, :] == ids, dot_of, 0.0), axis=0, keepdims=True
                )
            if w == 0 and i == 0:
                own[...] = value
            else:
                part[b] = value.astype(BF)
                for c in home_copies(b):
                    c.start()

    wpart[...] = jnp.zeros_like(wpart)
    waves = p.waves
    for step in range(waves + 3):
        if step < waves:
            fill(step)
            scatter(step)
        if 1 <= step <= waves:
            activate(step - 1)
        if 2 <= step <= waves + 1:
            forward(step - 2)
        if 3 <= step:
            send_home(step - 3)

    def stacked(strips):
        return join(strips, 0)

    def pile(ref, e):
        return stacked([ref[w, pl.ds(e * p.slots, p.slots), :] for w in range(waves)])

    def pile_acts(kind, e):
        return stacked([strip_of(w, kind, e) for w in range(waves)])

    ts[...] = jnp.zeros_like(ts)
    es[...] = jnp.zeros_like(es)
    for e in range(p.experts):
        down = dot(pile_acts(0, e), pile(weighted, e), 0, 0)
        down_out[e] = down
        ts[pl.ds(e, 1), :] = row_squares(down * down)
    so = stacked([shared_rows(w) for w in range(waves)])
    pair[0] = dot(so, stacked([wave_rows(w, all_x) for w in range(waves)]), 0, 0)
    pair[1] = dot(so, stacked([wave_rows(w, all_dy) for w in range(waves)]), 0, 0)
    for c in range(nc):
        size = min(p.cpc, p.cols - c * p.cpc)
        if size <= 0:
            continue
        to = pl.ds(c * p.cpc, size)
        sd_out[to, :] = pair[0 + 1, pl.ds(c * LANES, size), :]
        sg_out[to, :] = pair[0, pl.ds(c * LANES + p.cpc, size), :]
        su_out[to, :] = pair[0, pl.ds(c * LANES + 2 * p.cpc, size), :]
    sg, su, sd = sg_out[...], su_out[...], sd_out[...]
    es[0:1, :] = jnp.sum(sg * sg, axis=0, keepdims=True)
    es[1:2, :] = jnp.sum(su * su, axis=0, keepdims=True)
    ts[pl.ds(p.experts, 1), pl.ds(0, p.cols)] = row_squares(sd * sd)
    last = []
    for d, q in enumerate(eps):
        last.append(remote(es, es_in.at[d], e_s.at[d], e_r.at[d], {"ep": q}))
    for d, q in enumerate(tps):
        last.append(remote(ts, ts_in.at[d], t_s.at[d], t_r.at[d], {"tp": q}))
    for c in last:
        c.start()
    for e in range(p.experts):
        rows = pile(recv_x, e)
        gate = dot(rows, pile_acts(1, e), 0, 0)
        gate_out[e] = gate
        gate_sq[pl.ds(e, 1), :] = row_squares(gate * gate)
        up = dot(rows, pile_acts(2, e), 0, 0)
        up_out[e] = up
        up_sq[pl.ds(e, 1), :] = row_squares(up * up)

    total = own[...]
    w_total = wpart[ep]
    for b in eps:
        for ref, k in ((part_in, 0), (wpart_in, 1)):
            remote(ref.at[b], ref.at[b], r_s.at[b, k], r_r.at[b, k], {"ep": b}).wait_recv()
        total = total + part_in[b].astype(F32)
        w_total = w_total + wpart_in[b]
    token_out[...] = total.astype(BF)
    weight_out[...] = w_total[: p.picks]
    for c in last:
        c.wait_recv()
    norms = es[...]
    for d in range(n_ep - 1):
        norms = norms + es_in[d]
    sg_sq[...] = norms[0:1]
    su_sq[...] = norms[1:2]
    rows = ts[...]
    for d in range(n_tp - 1):
        rows = rows + ts_in[d]
    down_sq[...] = rows[: p.experts]
    sd_sq[...] = rows[p.experts : p.experts + 1, : p.cols]

    for cond, side, step in ((go_right, 0, 1), (go_left, 1, -1)):

        @pl.when(cond)
        def _(side=side, step=step):
            for k in range(3):
                relay(ep, k, zo.at[side, k], step).wait_send()

    for k in range(1, n_ep):
        b = order[k]

        @pl.when(((b < ep) & go_right) | ((b > ep) & go_left))
        def _(b=b):
            for a in range(3):
                relay(b, a, zs.at[b, a], 0).wait_send()

        for c in home_copies(b):
            c.wait_send()
    for w in range(waves):
        swap_copy(w).wait_send()
        for d in range(half - 1):
            scatter_copy(w, d).wait_send()
            gather_copy(w, d, place).wait_send()
        for d in range(half):
            side_copy(w, d, place).wait_send()
    for c in last:
        c.wait_send()


def copy_kernel(count, *refs):
    srcs, dsts, sem = refs[:count], refs[count : 2 * count], refs[2 * count]
    copies = [
        pltpu.make_async_copy(srcs[k], dsts[k], sem.at[k]) for k in range(count)
    ]
    for c in copies:
        c.start()
    for c in copies:
        c.wait()


def per_device(
    n_ep, n_tp,
    tokens, cotangent, routes, gate_weights,
    expert_gate, expert_up, expert_down,
    shared_gate, shared_up, shared_down,
):
    dma = pltpu.SemaphoreType.DMA
    vm = pltpu.VMEM
    tok, narrow = tokens.shape
    picks = routes.shape[1]
    experts, _, ff = expert_gate.shape
    p = Plan(n_ep, n_tp, tok, picks, narrow, experts, ff, shared_gate.shape[1])
    half, waves = p.half, p.waves
    meta_rows = up_to(2 * picks, 8)
    ts_rows = up_to(experts + 1, 8)
    wide = p.nc * LANES
    outs = [
        ((tok, narrow), BF), ((picks, tok), F32),
        ((experts, narrow, ff), F32), ((experts, narrow, ff), F32), ((experts, ff, narrow), F32),
        ((p.cols, narrow), F32), ((p.cols, narrow), F32), ((p.cols, narrow), F32),
        ((experts, narrow), F32), ((experts, narrow), F32), ((experts, ff), F32),
        ((1, narrow), F32), ((1, narrow), F32), ((1, p.cols), F32),
    ]
    out_shape = [jax.ShapeDtypeStruct(s, t) for s, t in outs]
    out_bytes = sum(
        up_to(s[-2], 8) * up_to(s[-1], LANES) * (s[0] if len(s) == 3 else 1) * jnp.dtype(t).itemsize
        for s, t in outs
    )
    grant = (VMEM_BYTES - out_bytes) // 2**18 * 2**18 - ROOM
    results = pl.pallas_call(
        functools.partial(main_kernel, p),
        out_shape=out_shape,
        in_specs=[HBM] * 10,
        out_specs=[VMEM] * len(outs),
        scratch_shapes=[
            vm(expert_gate.shape, BF), vm(expert_up.shape, BF), vm(expert_down.shape, BF),
            vm((p.cols, narrow), BF), vm((p.cols, narrow), BF), vm((p.cols, narrow), BF),
            vm((picks, tok), jnp.int32), vm((picks, tok), F32),
            vm((n_ep, tok, narrow), BF), vm((n_ep, tok, narrow), BF),
            vm((n_ep, meta_rows, tok), F32),
            vm((narrow, wide), BF), vm((narrow, wide), BF), vm((wide, narrow), BF),
            vm((waves, p.bpw, p.rows, tok), BF),
            vm((waves, p.rows, narrow), BF), vm((waves, p.rows, narrow), BF),
            vm((waves, p.rows, LANES), F32),
            vm((waves, 2, half, p.slab, LANES), F32),
            vm((waves, half, p.slab, LANES), F32),
            vm((waves, half, p.slab, LANES), BF),
            vm((waves, half - 1, p.slab, LANES), BF),
            vm((waves, n_tp, p.out_slab, LANES), BF),
            vm((2, wide, narrow), F32),
            vm((n_ep, tok, narrow), BF), vm((n_ep, tok, narrow), BF), vm((tok, narrow), F32),
            vm((n_ep, 8, tok), F32), vm((n_ep, 8, tok), F32),
            vm((ts_rows, ff), F32), vm((n_tp - 1, ts_rows, ff), F32),
            vm((8, narrow), F32), vm((n_ep - 1, 8, narrow), F32),
            dma((10,)), dma((2, 3)), dma((n_ep, 3)), dma((n_ep, 3)),
            dma((waves,)), dma((waves,)),
            dma((waves, half - 1)), dma((waves, half - 1)),
            dma((waves, half - 1)), dma((waves, half - 1)),
            dma((waves, half)), dma((waves, half)),
            dma((n_ep, 2)), dma((n_ep, 2)),
            dma((n_ep - 1,)), dma((n_ep - 1,)), dma((n_tp - 1,)), dma((n_tp - 1,)),
        ],
        compiler_params=pltpu.CompilerParams(
            collective_id=0, has_side_effects=True, vmem_limit_bytes=grant
        ),
    )(
        *[
            pltpu.with_memory_space_constraint(a, pltpu.HBM)
            for a in (
                tokens, cotangent, routes.T, gate_weights.T,
                expert_gate, expert_up, expert_down,
                shared_gate.T, shared_up.T, shared_down,
            )
        ]
    )
    count = len(outs)
    (
        token_grad, weight_grad, gate, up, down, sg, su, sd,
        gate_sq, up_sq, down_sq, sg_sq, su_sq, sd_sq,
    ) = pl.pallas_call(
        functools.partial(copy_kernel, count),
        out_shape=out_shape,
        in_specs=[VMEM] * count,
        out_specs=[HBM] * count,
        scratch_shapes=[dma((count,))],
        compiler_params=pltpu.CompilerParams(vmem_limit_bytes=20 * 1024 * 1024),
    )(*results)
    return (
        token_grad, weight_grad.T, gate, up, down, sg.T, su.T, sd,
        gate_sq, up_sq, down_sq, sg_sq[0], su_sq[0], sd_sq[0],
    )


def solution(mesh):
    n_ep, n_tp = mesh.shape["ep"], mesh.shape["tp"]
    return jax.shard_map(
        functools.partial(per_device, n_ep, n_tp),
        mesh=mesh,
        in_specs=(
            P("ep", "tp"),
            P("ep", "tp"),
            P("ep", None),
            P("ep", None),
            P("ep", "tp", None),
            P("ep", "tp", None),
            P("ep", None, "tp"),
            P("tp", None),
            P("tp", None),
            P(None, "tp"),
        ),
        out_specs=(
            P("ep", "tp"),
            P("ep", None),
            P("ep", "tp", None),
            P("ep", "tp", None),
            P("ep", None, "tp"),
            P("tp", "ep"),
            P("tp", "ep"),
            P("ep", "tp"),
            P("ep", "tp"),
            P("ep", "tp"),
            P("ep", None),
            P("tp"),
            P("tp"),
            P("ep"),
        ),
        check_vma=False,
    )
```

```python
import functools

import jax
import jax.numpy as jnp
from jax import lax
from jax.experimental import pallas as pl
from jax.experimental.pallas import tpu as pltpu
from jax.sharding import PartitionSpec as P

BF = jnp.bfloat16
F32 = jnp.float32
MESH = pl.DeviceIdType.MESH
VMEM = pl.BlockSpec(memory_space=pltpu.VMEM)
HBM = pl.BlockSpec(memory_space=pltpu.HBM)
LANES = 128
WAVE_ROWS = 16
VMEM_BYTES = 67_043_328
ROOM = 14 * 2**20


def up_to(value, unit):
    return (value + unit - 1) // unit * unit


def silu_parts(pre):
    logistic = jax.nn.sigmoid(pre)
    return (pre * logistic, logistic * (1.0 + pre * (1.0 - logistic)))


def remote(src, dst, send, recv, where):
    return pltpu.make_async_remote_copy(
        src_ref=src,
        dst_ref=dst,
        send_sem=send,
        recv_sem=recv,
        device_id=where,
        device_id_type=MESH,
    )


def dot(left, right, left_dim, right_dim, precision=None):
    return lax.dot_general(
        left,
        right,
        (((left_dim,), (right_dim,)), ((), ())),
        precision=precision,
        preferred_element_type=F32,
    )


def row_squares(square):
    ones = jnp.ones((8, square.shape[1]), BF)
    high = square.astype(BF)
    low = (square - high.astype(F32)).astype(BF)
    return (dot(ones, high, 1, 1) + dot(ones, low, 1, 1))[:1, :]


def join(parts, axis):
    return parts[0] if len(parts) == 1 else jnp.concatenate(parts, axis=axis)


def nearest(ep, n_ep, k):
    if k == 0:
        return ep
    left, right = ep, n_ep - 1 - ep
    both = jnp.minimum(left, right)
    paired = jnp.where(2 * both >= k, 1, 0)
    far = jnp.where(paired == 1, (k + 1) // 2, k - both)
    go_left = jnp.where(paired == 1, k % 2, jnp.where(left > right, 1, 0))
    return ep + far * (1 - 2 * go_left)


class Plan:
    def __init__(self, n_ep, n_tp, tok, picks, narrow, experts, ff, shared):
        self.n_ep, self.n_tp, self.tok, self.picks = n_ep, n_tp, tok, picks
        self.narrow, self.experts, self.ff = narrow, experts, ff
        all_experts = experts * n_ep
        self.capacity = max(2, (tok * picks + all_experts - 1) // all_experts)
        self.half = n_tp // 2
        self.nc = ff // LANES
        self.nr = self.half // self.nc
        self.bpw = max(
            b for b in range(1, n_ep + 1)
            if n_ep % b == 0 and (b == 1 or b * self.capacity <= WAVE_ROWS)
        )
        self.waves = n_ep // self.bpw
        self.slots = up_to(self.capacity * self.bpw, 16)
        self.rows = up_to(experts * self.slots, self.slots * 2 * self.nr)
        self.rc = self.rows // (2 * self.nr)
        self.wave_tok = self.bpw * tok
        self.sc = self.wave_tok // (2 * self.nr)
        self.cols = shared // n_ep
        self.cpc = -(-self.cols // self.nc)
        self.slab = 3 * self.rc + self.sc
        self.out_slab = self.slab + 16
        self.e_rows = up_to(experts, 8)
        assert self.half % self.nc == 0 and self.nr > 0 and self.rc <= LANES
        assert self.sc % 16 == 0 and 3 * self.cpc <= LANES

    def place(self, q, c):
        return (q // self.nr) * self.half + (q % self.nr) * self.nc + c

    def strip(self, index):
        row = index * self.slots
        return row // self.rc, row % self.rc


def main_kernel(
    p,
    x, dy, routes, weights, w_gate, w_up, w_down, sg_w, su_w, sd_w,
    token_out, weight_out, gate_out, up_out, down_out, sg_out, su_out, sd_out,
    gate_sq, up_sq, down_sq, sg_sq, su_sq, sd_sq,
    wg, wu, wd, sgv, suv, sdv, rts, gws, all_x, all_dy, all_meta,
    s_in, s_back, s_out_w, oh, recv_x, weighted, rw,
    full, got, held, landed, acts, pair, part, part_in, own, wpart, wpart_in,
    ts, ts_in, es, es_in,
    ld, zo, zs, zr, a_s, a_r, b_s, b_r, c_s, c_r, d_s, d_r, r_s, r_r, e_s, e_r, t_s, t_r,
):
    n_ep, n_tp, half, nc, nr = p.n_ep, p.n_tp, p.half, p.nc, p.nr
    ep, me = lax.axis_index("ep"), lax.axis_index("tp")
    parity = lax.rem(me, 2)
    mine = me // 2
    partner = {"tp": me + 1 - 2 * parity}
    others = [lax.rem(mine + d, half) for d in range(1, half)]
    places = [{"tp": 2 * j + parity} for j in others]
    eps = [lax.rem(ep + d, n_ep) for d in range(1, n_ep)]
    tps = [lax.rem(me + d, n_tp) for d in range(1, n_tp)]
    arrival = [nearest(ep, n_ep, k) for k in range(n_ep)]
    order = list(arrival)
    if n_ep == 4:
        middle = (ep == 1) | (ep == 2)
        order[2] = jnp.where(middle, arrival[3], arrival[2])
        order[3] = jnp.where(middle, arrival[2], arrival[3])
    place = parity * half + mine

    barrier = pltpu.get_barrier_semaphore()
    for where in [{"ep": q} for q in eps] + [{"tp": q} for q in tps]:
        pl.semaphore_signal(barrier, inc=1, device_id=where, device_id_type=MESH)

    span = pl.ds(pl.multiple_of(ep * p.cols, 8), p.cols)
    sources = (
        (x, all_x.at[ep]), (dy, all_dy.at[ep]), (routes, rts), (weights, gws),
        (sg_w.at[span], sgv), (su_w.at[span], suv), (sd_w.at[span], sdv),
        (w_gate, wg), (w_up, wu), (w_down, wd),
    )
    loads = []
    for k, (src, dst) in enumerate(sources):
        loads.append(pltpu.make_async_copy(src, dst, ld.at[k]))
        loads[-1].start()

    loads[2].wait()
    loads[3].wait()
    all_meta[ep] = jnp.concatenate(
        [rts[...].astype(F32), gws[...]]
        + [jnp.zeros((all_meta.shape[1] - 2 * p.picks, p.tok), F32)] * (
            all_meta.shape[1] > 2 * p.picks
        ),
        axis=0,
    )
    loads[0].wait()
    loads[1].wait()

    blocks = (all_meta, all_x, all_dy)

    def relay(b, k, send, step):
        return remote(
            blocks[k].at[b], blocks[k].at[b], send, zr.at[b, k], {"ep": ep + step}
        )

    go_right, go_left = ep < n_ep - 1, ep > 0

    def send_own():
        for cond, side, step in ((go_right, 0, 1), (go_left, 1, -1)):

            @pl.when(cond)
            def _(side=side, step=step):
                for k in range(3):
                    relay(ep, k, zo.at[side, k], step).start()

    def arrive(k, arrays):
        b = arrival[k]
        for a in arrays:
            relay(b, a, zs.at[b, a], 0).wait_recv()

            @pl.when((b < ep) & go_right)
            def _(a=a):
                relay(b, a, zs.at[b, a], 1).start()

            @pl.when((b > ep) & go_left)
            def _(a=a):
                relay(b, a, zs.at[b, a], -1).start()

    reach = 2 * jnp.minimum(ep, n_ep - 1 - ep)

    def take(j, arrays):
        for k in range(max(j, 1), min(j + 3, n_ep)):
            early = k - 1 if k % 2 else max(1, k - 2)
            if k == 1:
                if j == 1:
                    arrive(k, arrays)
            elif j == early or j == k:
                inside = reach >= k - k % 2

                @pl.when(inside if j == early else jnp.logical_not(inside))
                def _(k=k):
                    arrive(k, arrays)

    def take_wave(w, arrays):
        for i in range(p.bpw):
            take(w * p.bpw + i, arrays)

    lane_n = lax.broadcasted_iota(jnp.int32, (p.cols, nc * LANES), 1)
    row_i = lax.broadcasted_iota(jnp.int32, (p.cols, nc * LANES), 0)
    chunk = lax.shift_right_logical(lane_n, 7)
    lane = lane_n - chunk * LANES

    def spread_map(k):
        inside = (lane >= k * p.cpc) & (lane < (k + 1) * p.cpc)
        same = row_i == chunk * p.cpc + lane - k * p.cpc
        return jnp.where(inside & same, 1.0, 0.0).astype(BF)

    for k in range(4, 7):
        loads[k].wait()
    maps = [spread_map(k) for k in range(3)]
    s_in[...] = (dot(sgv[...], maps[0], 0, 0) + dot(suv[...], maps[1], 0, 0)).astype(BF)
    s_back[...] = dot(sdv[...], maps[2], 0, 0).astype(BF)
    s_out_w[...] = (dot(maps[1], sgv[...], 0, 0) + dot(maps[2], suv[...], 0, 0)).astype(BF)

    ids = (
        ep * p.experts + lax.broadcasted_iota(jnp.int32, (p.e_rows, p.tok), 0)
    ).astype(F32)
    before = jnp.where(
        lax.broadcasted_iota(jnp.int32, (p.tok, p.tok), 0)
        < lax.broadcasted_iota(jnp.int32, (p.tok, p.tok), 1),
        1.0,
        0.0,
    ).astype(BF)
    place_in = lax.broadcasted_iota(jnp.int32, (p.slots, p.tok), 0).astype(F32)
    spare = p.rows - p.experts * p.slots

    def route(w):
        sums = [jnp.zeros((p.slots, 1), F32) for _ in range(p.experts)]
        for i in range(p.bpw):
            info = all_meta[order[w * p.bpw + i]]
            chosen = jnp.zeros((p.e_rows, p.tok), F32)
            weight_of = jnp.zeros((p.e_rows, p.tok), F32)
            for k in range(p.picks):
                same = info[k : k + 1, :] == ids
                chosen = jnp.where(same, 1.0, chosen)
                weight_of = jnp.where(
                    same, info[p.picks + k : p.picks + k + 1, :], weight_of
                )
            rank = dot(chosen.astype(BF), before, 1, 0)
            slot = jnp.where(chosen > 0.0, rank + float(p.capacity * i), -1.0)
            for e in range(p.experts):
                hot = place_in == slot[e : e + 1, :]
                oh[w, i, pl.ds(e * p.slots, p.slots), :] = jnp.where(hot, 1.0, 0.0).astype(BF)
                sums[e] = sums[e] + jnp.sum(
                    jnp.where(hot, weight_of[e : e + 1, :], 0.0), axis=1, keepdims=True
                )
            if spare:
                oh[w, i, pl.ds(p.experts * p.slots, spare), :] = jnp.zeros((spare, p.tok), BF)
        for e in range(p.experts):
            rw[w, pl.ds(e * p.slots, p.slots), :] = jnp.broadcast_to(sums[e], (p.slots, LANES))
        if spare:
            rw[w, pl.ds(p.experts * p.slots, spare), :] = jnp.zeros((spare, LANES), F32)

    def pick(w, source):
        total = dot(oh[w, 0], source[order[w * p.bpw]], 1, 0)
        for i in range(1, p.bpw):
            total = total + dot(oh[w, i], source[order[w * p.bpw + i]], 1, 0)
        return total

    def wave_rows(w, source):
        return join([source[order[w * p.bpw + i]] for i in range(p.bpw)], 0)

    def swap_copy(w):
        return remote(full.at[w, 1 - parity], got.at[w], a_s.at[w], a_r.at[w], partner)

    def put(w, e, kind, value):
        q, at = p.strip(e)
        for c in range(nc):
            full[
                w, q // nr, (q % nr) * nc + c, pl.ds(kind * p.rc + at, p.slots), :
            ] = value[:, c * LANES : (c + 1) * LANES]

    def fill(w):
        if w == 0 and p.bpw > 1:
            take_wave(0, (0, 1))
        if w > 0 or p.bpw > 1:
            route(w)
            recv_x[w] = pick(w, all_x).astype(BF)
        if w == 0:
            loads[7].wait()
            loads[8].wait()
        for kind, weight in ((0, wg), (1, wu)):
            for e in range(p.experts):
                put(w, e, kind, dot(recv_x[w, pl.ds(e * p.slots, p.slots), :], weight[e], 1, 0))
        take_wave(w, (2,))
        recv_dy = pick(w, all_dy)
        weighted[w] = (rw[w][:, :1] * recv_dy).astype(BF)
        narrow_dy = recv_dy.astype(BF)
        if w == 0:
            loads[9].wait()
        for e in range(p.experts):
            put(w, e, 2, dot(narrow_dy[e * p.slots : (e + 1) * p.slots, :], wd[e], 1, 1))
        for s in range(p.experts, p.rows // p.slots):
            for kind in range(3):
                put(w, s, kind, jnp.zeros((p.slots, p.ff), F32))
        s = dot(wave_rows(w, all_x), s_in[...], 1, 0) + dot(
            wave_rows(w, all_dy), s_back[...], 1, 0
        )
        for q in range(2 * nr):
            for c in range(nc):
                full[w, q // nr, (q % nr) * nc + c, pl.ds(3 * p.rc, p.sc), :] = s[
                    q * p.sc : (q + 1) * p.sc, c * LANES : (c + 1) * LANES
                ]
        swap_copy(w).start()

    def scatter_copy(w, d):
        return remote(
            held.at[w, others[d]], landed.at[w, d], b_s.at[w, d], b_r.at[w, d], places[d]
        )

    def scatter(w):
        swap_copy(w).wait_recv()
        for d, j in enumerate(others):
            held[w, j] = (full[w, parity, j] + got[w, j]).astype(BF)
            scatter_copy(w, d).start()

    def gather_copy(w, d, block):
        ref = acts.at[w, block]
        return remote(ref, ref, c_s.at[w, d], c_r.at[w, d], places[d])

    def side_copy(w, d, block):
        ref = acts.at[w, block]
        return remote(ref, ref, d_s.at[w, d], d_r.at[w, d], partner)

    def activate(w):
        out = full[w, parity, mine] + got[w, mine]
        for d in range(half - 1):
            scatter_copy(w, d).wait_recv()
            out = out + landed[w, d].astype(F32)
        gate, up, back = (out[k * p.rc : (k + 1) * p.rc] for k in range(3))
        silu_out, silu_slope = silu_parts(gate)
        hidden = (silu_out * up).astype(BF)
        band = parity * nr + mine // nc
        weight = rw[w, pl.ds(pl.multiple_of(band * p.rc, p.rc), p.rc), :]
        dhidden = weight * back
        acts[w, place, pl.ds(0, p.rc), :] = hidden
        acts[w, place, pl.ds(p.rc, p.rc), :] = (dhidden * up * silu_slope).astype(BF)
        acts[w, place, pl.ds(2 * p.rc, p.rc), :] = (dhidden * silu_out).astype(BF)
        dots = dot(
            jnp.ones((16, LANES), F32), hidden.astype(F32) * back, 1, 1, lax.Precision.HIGHEST
        )
        high = dots.astype(BF).astype(F32)
        mid = (dots - high).astype(BF).astype(F32)
        low = dots - high - mid
        line = lax.broadcasted_iota(jnp.int32, dots.shape, 0)
        pieces = jnp.where(line == 0, high, jnp.where(line == 1, mid, low))
        acts[w, place, pl.ds(3 * p.rc, 16), pl.ds(0, p.rc)] = pieces.astype(BF)
        both = out[3 * p.rc :]
        at = lax.broadcasted_iota(jnp.int32, both.shape, 1)
        s_up = pltpu.roll(both, LANES - p.cpc, 1)
        s_bk = pltpu.roll(both, LANES - 2 * p.cpc, 1)
        s_out, s_slope = silu_parts(both)
        s_dgate = pltpu.roll(s_bk * s_up * s_slope, p.cpc, 1)
        s_dup = pltpu.roll(s_bk * s_out, 2 * p.cpc, 1)
        value = jnp.where(
            at < p.cpc,
            s_out * s_up,
            jnp.where(at < 2 * p.cpc, s_dgate, jnp.where(at < 3 * p.cpc, s_dup, 0.0)),
        )
        acts[w, place, pl.ds(3 * p.rc + 16, p.sc), :] = value.astype(BF)
        for d in range(half - 1):
            gather_copy(w, d, place).start()
        side_copy(w, 0, place).start()

    def origin(d):
        return lax.rem(mine + half - 1 - d, half)

    def forward(w):
        for d in range(half - 1):
            block = parity * half + origin(d)
            gather_copy(w, d, block).wait_recv()
            side_copy(w, 1 + d, block).start()

    def strip_of(w, kind, e):
        q, at = p.strip(e)
        return join(
            [acts[w, p.place(q, c), pl.ds(kind * p.rc + at, p.slots), :] for c in range(nc)], 1
        )

    def shared_rows(w):
        return join(
            [
                join(
                    [
                        acts[w, p.place(q, c), pl.ds(3 * p.rc + 16, p.sc), :]
                        for c in range(nc)
                    ],
                    1,
                )
                for q in range(2 * nr)
            ],
            0,
        )

    def home_copies(b):
        return (
            remote(part.at[b], part_in.at[ep], r_s.at[b, 0], r_r.at[ep, 0], {"ep": b}),
            remote(wpart.at[b], wpart_in.at[ep], r_s.at[b, 1], r_r.at[ep, 1], {"ep": b}),
        )

    def send_home(w):
        side_copy(w, 0, (1 - parity) * half + mine).wait_recv()
        for d in range(half - 1):
            side_copy(w, 1 + d, (1 - parity) * half + origin(d)).wait_recv()
        row_grad = []
        for e in range(p.experts):
            row_grad.append(
                (
                    dot(strip_of(w, 1, e), wg[e], 1, 1) + dot(strip_of(w, 2, e), wu[e], 1, 1)
                ).astype(BF)
            )
        if spare:
            row_grad.append(jnp.zeros((spare, p.narrow), BF))
        row_grad = join(row_grad, 0)
        s_grad = dot(shared_rows(w), s_out_w[...], 1, 0)
        row_e = lax.broadcasted_iota(jnp.int32, (p.e_rows, p.rc), 0)
        row_l = lax.broadcasted_iota(jnp.int32, (p.e_rows, p.rc), 1)
        masked = []
        for q in range(2 * nr):
            line = jnp.zeros((1, p.rc), F32)
            for c in range(nc):
                pieces = acts[w, p.place(q, c), pl.ds(3 * p.rc, 16), pl.ds(0, p.rc)].astype(F32)
                line = line + (pieces[0:1] + pieces[1:2] + pieces[2:3])
            row = row_l + q * p.rc
            inside = (row >= row_e * p.slots) & (row < (row_e + 1) * p.slots)
            masked.append(jnp.where(inside, line, 0.0))
        for i in range(p.bpw):
            b = order[w * p.bpw + i]
            value = dot(oh[w, i], row_grad, 0, 0) + s_grad[i * p.tok : (i + 1) * p.tok, :]

            info = all_meta[b]
            dot_of = jnp.zeros((p.e_rows, p.tok), F32)
            for q in range(2 * nr):
                dot_of = dot_of + dot(
                    masked[q], oh[w, i, pl.ds(q * p.rc, p.rc), :].astype(F32), 1, 0,
                    lax.Precision.HIGHEST,
                )
            for k in range(p.picks):
                wpart[b, pl.ds(k, 1), :] = jnp.sum(
                    jnp.where(info[k : k + 1, :] == ids, dot_of, 0.0), axis=0, keepdims=True
                )
            if w == 0 and i == 0:
                own[...] = value
            else:
                part[b] = value.astype(BF)
                for c in home_copies(b):
                    c.start()

    wpart[...] = jnp.zeros_like(wpart)
    waves = p.waves
    if p.bpw == 1:
        route(0)
        recv_x[0] = pick(0, all_x).astype(BF)
    pl.semaphore_wait(barrier, n_ep + n_tp - 2)
    send_own()
    for step in range(waves):
        fill(step)
        scatter(step)
        if step + 1 < waves:
            take_wave(step + 1, (0, 1))
        if step >= 3:
            forward(step - 3)
        if step >= 1:
            activate(step - 1)
        if step >= 4:
            send_home(step - 4)
    late = max(0, waves - 3)
    if waves > 2:
        forward(late)
        for w in range(max(0, waves - 4), late + 1):
            send_home(w)
        late = late + 1
    activate(waves - 1)
    for w in range(late, waves):
        forward(w)
        send_home(w)

    def stacked(strips):
        return join(strips, 0)

    def pile(ref, e):
        return stacked([ref[w, pl.ds(e * p.slots, p.slots), :] for w in range(waves)])

    def pile_acts(kind, e):
        return stacked([strip_of(w, kind, e) for w in range(waves)])

    ts[...] = jnp.zeros_like(ts)
    es[...] = jnp.zeros_like(es)
    for e in range(p.experts):
        down = dot(pile_acts(0, e), pile(weighted, e), 0, 0)
        down_out[e] = down
        ts[pl.ds(e, 1), :] = row_squares(down * down)
    so = stacked([shared_rows(w) for w in range(waves)])
    pair[0] = dot(so, stacked([wave_rows(w, all_x) for w in range(waves)]), 0, 0)
    pair[1] = dot(so, stacked([wave_rows(w, all_dy) for w in range(waves)]), 0, 0)
    for c in range(nc):
        size = min(p.cpc, p.cols - c * p.cpc)
        if size <= 0:
            continue
        to = pl.ds(c * p.cpc, size)
        sd_out[to, :] = pair[0 + 1, pl.ds(c * LANES, size), :]
        sg_out[to, :] = pair[0, pl.ds(c * LANES + p.cpc, size), :]
        su_out[to, :] = pair[0, pl.ds(c * LANES + 2 * p.cpc, size), :]
    sg, su, sd = sg_out[...], su_out[...], sd_out[...]
    es[0:1, :] = jnp.sum(sg * sg, axis=0, keepdims=True)
    es[1:2, :] = jnp.sum(su * su, axis=0, keepdims=True)
    ts[pl.ds(p.experts, 1), pl.ds(0, p.cols)] = row_squares(sd * sd)
    last = []
    for d, q in enumerate(eps):
        last.append(remote(es, es_in.at[d], e_s.at[d], e_r.at[d], {"ep": q}))
    for d, q in enumerate(tps):
        last.append(remote(ts, ts_in.at[d], t_s.at[d], t_r.at[d], {"tp": q}))
    for c in last:
        c.start()
    for e in range(p.experts):
        rows = pile(recv_x, e)
        gate = dot(rows, pile_acts(1, e), 0, 0)
        gate_out[e] = gate
        gate_sq[pl.ds(e, 1), :] = row_squares(gate * gate)
        up = dot(rows, pile_acts(2, e), 0, 0)
        up_out[e] = up
        up_sq[pl.ds(e, 1), :] = row_squares(up * up)

    total = own[...]
    w_total = wpart[ep]
    for b in eps:
        for ref, k in ((part_in, 0), (wpart_in, 1)):
            remote(ref.at[b], ref.at[b], r_s.at[b, k], r_r.at[b, k], {"ep": b}).wait_recv()
        total = total + part_in[b].astype(F32)
        w_total = w_total + wpart_in[b]
    token_out[...] = total.astype(BF)
    weight_out[...] = w_total[: p.picks]
    for c in last:
        c.wait_recv()
    norms = es[...]
    for d in range(n_ep - 1):
        norms = norms + es_in[d]
    sg_sq[...] = norms[0:1]
    su_sq[...] = norms[1:2]
    rows = ts[...]
    for d in range(n_tp - 1):
        rows = rows + ts_in[d]
    down_sq[...] = rows[: p.experts]
    sd_sq[...] = rows[p.experts : p.experts + 1, : p.cols]

    for cond, side, step in ((go_right, 0, 1), (go_left, 1, -1)):

        @pl.when(cond)
        def _(side=side, step=step):
            for k in range(3):
                relay(ep, k, zo.at[side, k], step).wait_send()

    for k in range(1, n_ep):
        b = order[k]

        @pl.when(((b < ep) & go_right) | ((b > ep) & go_left))
        def _(b=b):
            for a in range(3):
                relay(b, a, zs.at[b, a], 0).wait_send()

        for c in home_copies(b):
            c.wait_send()
    for w in range(waves):
        swap_copy(w).wait_send()
        for d in range(half - 1):
            scatter_copy(w, d).wait_send()
            gather_copy(w, d, place).wait_send()
        for d in range(half):
            side_copy(w, d, place).wait_send()
    for c in last:
        c.wait_send()


def copy_kernel(count, *refs):
    srcs, dsts, sem = refs[:count], refs[count : 2 * count], refs[2 * count]
    copies = [
        pltpu.make_async_copy(srcs[k], dsts[k], sem.at[k]) for k in range(count)
    ]
    for c in copies:
        c.start()
    for c in copies:
        c.wait()


def per_device(
    n_ep, n_tp,
    tokens, cotangent, routes, gate_weights,
    expert_gate, expert_up, expert_down,
    shared_gate, shared_up, shared_down,
):
    dma = pltpu.SemaphoreType.DMA
    vm = pltpu.VMEM
    tok, narrow = tokens.shape
    picks = routes.shape[1]
    experts, _, ff = expert_gate.shape
    p = Plan(n_ep, n_tp, tok, picks, narrow, experts, ff, shared_gate.shape[1])
    half, waves = p.half, p.waves
    meta_rows = up_to(2 * picks, 8)
    ts_rows = up_to(experts + 1, 8)
    wide = p.nc * LANES
    outs = [
        ((tok, narrow), BF), ((picks, tok), F32),
        ((experts, narrow, ff), F32), ((experts, narrow, ff), F32), ((experts, ff, narrow), F32),
        ((p.cols, narrow), F32), ((p.cols, narrow), F32), ((p.cols, narrow), F32),
        ((experts, narrow), F32), ((experts, narrow), F32), ((experts, ff), F32),
        ((1, narrow), F32), ((1, narrow), F32), ((1, p.cols), F32),
    ]
    out_shape = [jax.ShapeDtypeStruct(s, t) for s, t in outs]
    out_bytes = sum(
        up_to(s[-2], 8) * up_to(s[-1], LANES) * (s[0] if len(s) == 3 else 1) * jnp.dtype(t).itemsize
        for s, t in outs
    )
    grant = (VMEM_BYTES - out_bytes) // 2**18 * 2**18 - ROOM
    results = pl.pallas_call(
        functools.partial(main_kernel, p),
        out_shape=out_shape,
        in_specs=[HBM] * 10,
        out_specs=[VMEM] * len(outs),
        scratch_shapes=[
            vm(expert_gate.shape, BF), vm(expert_up.shape, BF), vm(expert_down.shape, BF),
            vm((p.cols, narrow), BF), vm((p.cols, narrow), BF), vm((p.cols, narrow), BF),
            vm((picks, tok), jnp.int32), vm((picks, tok), F32),
            vm((n_ep, tok, narrow), BF), vm((n_ep, tok, narrow), BF),
            vm((n_ep, meta_rows, tok), F32),
            vm((narrow, wide), BF), vm((narrow, wide), BF), vm((wide, narrow), BF),
            vm((waves, p.bpw, p.rows, tok), BF),
            vm((waves, p.rows, narrow), BF), vm((waves, p.rows, narrow), BF),
            vm((waves, p.rows, LANES), F32),
            vm((waves, 2, half, p.slab, LANES), F32),
            vm((waves, half, p.slab, LANES), F32),
            vm((waves, half, p.slab, LANES), BF),
            vm((waves, half - 1, p.slab, LANES), BF),
            vm((waves, n_tp, p.out_slab, LANES), BF),
            vm((2, wide, narrow), F32),
            vm((n_ep, tok, narrow), BF), vm((n_ep, tok, narrow), BF), vm((tok, narrow), F32),
            vm((n_ep, 8, tok), F32), vm((n_ep, 8, tok), F32),
            vm((ts_rows, ff), F32), vm((n_tp - 1, ts_rows, ff), F32),
            vm((8, narrow), F32), vm((n_ep - 1, 8, narrow), F32),
            dma((10,)), dma((2, 3)), dma((n_ep, 3)), dma((n_ep, 3)),
            dma((waves,)), dma((waves,)),
            dma((waves, half - 1)), dma((waves, half - 1)),
            dma((waves, half - 1)), dma((waves, half - 1)),
            dma((waves, half)), dma((waves, half)),
            dma((n_ep, 2)), dma((n_ep, 2)),
            dma((n_ep - 1,)), dma((n_ep - 1,)), dma((n_tp - 1,)), dma((n_tp - 1,)),
        ],
        compiler_params=pltpu.CompilerParams(
            collective_id=0, has_side_effects=True, vmem_limit_bytes=grant
        ),
    )(
        *[
            pltpu.with_memory_space_constraint(a, pltpu.HBM)
            for a in (
                tokens, cotangent, routes.T, gate_weights.T,
                expert_gate, expert_up, expert_down,
                shared_gate.T, shared_up.T, shared_down,
            )
        ]
    )
    count = len(outs)
    (
        token_grad, weight_grad, gate, up, down, sg, su, sd,
        gate_sq, up_sq, down_sq, sg_sq, su_sq, sd_sq,
    ) = pl.pallas_call(
        functools.partial(copy_kernel, count),
        out_shape=out_shape,
        in_specs=[VMEM] * count,
        out_specs=[HBM] * count,
        scratch_shapes=[dma((count,))],
        compiler_params=pltpu.CompilerParams(vmem_limit_bytes=20 * 1024 * 1024),
    )(*results)
    return (
        token_grad, weight_grad.T, gate, up, down, sg.T, su.T, sd,
        gate_sq, up_sq, down_sq, sg_sq[0], su_sq[0], sd_sq[0],
    )


def solution(mesh):
    n_ep, n_tp = mesh.shape["ep"], mesh.shape["tp"]
    return jax.shard_map(
        functools.partial(per_device, n_ep, n_tp),
        mesh=mesh,
        in_specs=(
            P("ep", "tp"),
            P("ep", "tp"),
            P("ep", None),
            P("ep", None),
            P("ep", "tp", None),
            P("ep", "tp", None),
            P("ep", None, "tp"),
            P("tp", None),
            P("tp", None),
            P(None, "tp"),
        ),
        out_specs=(
            P("ep", "tp"),
            P("ep", None),
            P("ep", "tp", None),
            P("ep", "tp", None),
            P("ep", None, "tp"),
            P("tp", "ep"),
            P("tp", "ep"),
            P("ep", "tp"),
            P("ep", "tp"),
            P("ep", "tp"),
            P("ep", None),
            P("tp"),
            P("tp"),
            P("ep"),
        ),
        check_vma=False,
    )
```

```python
import functools

import jax
import jax.numpy as jnp
from jax import lax
from jax.experimental import pallas as pl
from jax.experimental.pallas import tpu as pltpu
from jax.sharding import PartitionSpec as P

BF = jnp.bfloat16
F32 = jnp.float32
MESH = pl.DeviceIdType.MESH
VMEM = pl.BlockSpec(memory_space=pltpu.VMEM)
HBM = pl.BlockSpec(memory_space=pltpu.HBM)
LANES = 128
WAVE_ROWS = 16
VMEM_BYTES = 67_043_328
ROOM = 14 * 2**20


def up_to(value, unit):
    return (value + unit - 1) // unit * unit


def silu_parts(pre):
    logistic = jax.nn.sigmoid(pre)
    return (pre * logistic, logistic * (1.0 + pre * (1.0 - logistic)))


def remote(src, dst, send, recv, where):
    return pltpu.make_async_remote_copy(
        src_ref=src,
        dst_ref=dst,
        send_sem=send,
        recv_sem=recv,
        device_id=where,
        device_id_type=MESH,
    )


def dot(left, right, left_dim, right_dim, precision=None):
    return lax.dot_general(
        left,
        right,
        (((left_dim,), (right_dim,)), ((), ())),
        precision=precision,
        preferred_element_type=F32,
    )


def row_squares(square):
    ones = jnp.ones((8, square.shape[1]), BF)
    high = square.astype(BF)
    low = (square - high.astype(F32)).astype(BF)
    return (dot(ones, high, 1, 1) + dot(ones, low, 1, 1))[:1, :]


def join(parts, axis):
    return parts[0] if len(parts) == 1 else jnp.concatenate(parts, axis=axis)


def nearest(ep, n_ep, k):
    if k == 0:
        return ep
    left, right = ep, n_ep - 1 - ep
    both = jnp.minimum(left, right)
    paired = jnp.where(2 * both >= k, 1, 0)
    far = jnp.where(paired == 1, (k + 1) // 2, k - both)
    go_left = jnp.where(paired == 1, k % 2, jnp.where(left > right, 1, 0))
    return ep + far * (1 - 2 * go_left)


class Plan:
    def __init__(self, n_ep, n_tp, tok, picks, narrow, experts, ff, shared):
        self.n_ep, self.n_tp, self.tok, self.picks = n_ep, n_tp, tok, picks
        self.narrow, self.experts, self.ff = narrow, experts, ff
        all_experts = experts * n_ep
        self.capacity = max(2, (tok * picks + all_experts - 1) // all_experts)
        self.half = n_tp // 2
        self.nc = ff // LANES
        self.nr = self.half // self.nc
        self.bpw = max(
            b for b in range(1, n_ep + 1)
            if n_ep % b == 0 and (b == 1 or b * self.capacity <= WAVE_ROWS)
        )
        self.waves = n_ep // self.bpw
        self.slots = up_to(self.capacity * self.bpw, 16)
        self.rows = up_to(experts * self.slots, self.slots * 2 * self.nr)
        self.rc = self.rows // (2 * self.nr)
        self.wave_tok = self.bpw * tok
        self.sc = self.wave_tok // (2 * self.nr)
        self.cols = shared // n_ep
        self.cpc = -(-self.cols // self.nc)
        self.slab = 3 * self.rc + self.sc
        self.shared_at = 2 * self.rc + 16
        self.first = self.shared_at + self.sc
        self.out_slab = self.first + self.rc
        self.e_rows = up_to(experts, 8)
        assert self.half % self.nc == 0 and self.nr > 0 and self.rc <= LANES
        assert self.sc % 16 == 0 and 3 * self.cpc <= LANES

    def place(self, q, c):
        return (q // self.nr) * self.half + (q % self.nr) * self.nc + c

    def strip(self, index):
        row = index * self.slots
        return row // self.rc, row % self.rc


def main_kernel(
    p,
    x, dy, routes, weights, w_gate, w_up, w_down, sg_w, su_w, sd_w,
    token_out, weight_out, gate_out, up_out, down_out, sg_out, su_out, sd_out,
    gate_sq, up_sq, down_sq, sg_sq, su_sq, sd_sq,
    wg, wu, wd, sgv, suv, sdv, rts, gws, all_x, all_dy, all_meta,
    s_in, s_back, s_out_w, oh, recv_x, weighted, rw,
    full, got, held, landed, acts, pair, part, part_in, own, wpart, wpart_in,
    ts, ts_in, es, es_in,
    ld, zo, zs, zr, a_s, a_r, b_s, b_r, c_s, c_r, d_s, d_r, r_s, r_r, e_s, e_r, t_s, t_r,
    h_s, h_r,
):
    n_ep, n_tp, half, nc, nr = p.n_ep, p.n_tp, p.half, p.nc, p.nr
    ep, me = lax.axis_index("ep"), lax.axis_index("tp")
    parity = lax.rem(me, 2)
    mine = me // 2
    partner = {"tp": me + 1 - 2 * parity}
    if half == 4:
        flip_x = mine + 1 - 2 * lax.rem(mine, 2)
        flip_y = mine + 2 - 4 * (mine // 2)
        others = [3 - mine, flip_y, flip_x]
        origins = others
    else:
        others = [lax.rem(mine + d, half) for d in range(1, half)]
        origins = [lax.rem(mine + half - d, half) for d in range(1, half)]
    places = [{"tp": 2 * j + parity} for j in others]
    eps = [lax.rem(ep + d, n_ep) for d in range(1, n_ep)]
    tps = [lax.rem(me + d, n_tp) for d in range(1, n_tp)]
    arrival = [nearest(ep, n_ep, k) for k in range(n_ep)]
    order = list(arrival)
    if n_ep == 4:
        middle = (ep == 1) | (ep == 2)
        order[2] = jnp.where(middle, arrival[3], arrival[2])
        order[3] = jnp.where(middle, arrival[2], arrival[3])
    place = parity * half + mine

    barrier = pltpu.get_barrier_semaphore()
    for where in [{"ep": q} for q in eps] + [{"tp": q} for q in tps]:
        pl.semaphore_signal(barrier, inc=1, device_id=where, device_id_type=MESH)

    span = pl.ds(pl.multiple_of(ep * p.cols, 8), p.cols)
    sources = (
        (x, all_x.at[ep]), (dy, all_dy.at[ep]), (routes, rts), (weights, gws),
        (sg_w.at[span], sgv), (su_w.at[span], suv), (sd_w.at[span], sdv),
        (w_gate, wg), (w_up, wu), (w_down, wd),
    )
    loads = []
    for k, (src, dst) in enumerate(sources):
        loads.append(pltpu.make_async_copy(src, dst, ld.at[k]))
        loads[-1].start()

    loads[2].wait()
    loads[3].wait()
    all_meta[ep] = jnp.concatenate(
        [rts[...].astype(F32), gws[...]]
        + [jnp.zeros((all_meta.shape[1] - 2 * p.picks, p.tok), F32)] * (
            all_meta.shape[1] > 2 * p.picks
        ),
        axis=0,
    )
    loads[0].wait()
    loads[1].wait()

    blocks = (all_meta, all_x, all_dy)

    def relay(b, k, send, step):
        return remote(
            blocks[k].at[b], blocks[k].at[b], send, zr.at[b, k], {"ep": ep + step}
        )

    go_right, go_left = ep < n_ep - 1, ep > 0

    def send_own():
        for cond, side, step in ((go_right, 0, 1), (go_left, 1, -1)):

            @pl.when(cond)
            def _(side=side, step=step):
                for k in range(3):
                    relay(ep, k, zo.at[side, k], step).start()

    def arrive(k, arrays):
        b = arrival[k]
        for a in arrays:
            relay(b, a, zs.at[b, a], 0).wait_recv()

            @pl.when((b < ep) & go_right)
            def _(a=a):
                relay(b, a, zs.at[b, a], 1).start()

            @pl.when((b > ep) & go_left)
            def _(a=a):
                relay(b, a, zs.at[b, a], -1).start()

    reach = 2 * jnp.minimum(ep, n_ep - 1 - ep)

    def take(j, arrays):
        for k in range(max(j, 1), min(j + 3, n_ep)):
            early = k - 1 if k % 2 else max(1, k - 2)
            if k == 1:
                if j == 1:
                    arrive(k, arrays)
            elif j == early or j == k:
                inside = reach >= k - k % 2

                @pl.when(inside if j == early else jnp.logical_not(inside))
                def _(k=k):
                    arrive(k, arrays)

    def take_wave(w, arrays):
        for i in range(p.bpw):
            take(w * p.bpw + i, arrays)

    lane_n = lax.broadcasted_iota(jnp.int32, (p.cols, nc * LANES), 1)
    row_i = lax.broadcasted_iota(jnp.int32, (p.cols, nc * LANES), 0)
    chunk = lax.shift_right_logical(lane_n, 7)
    lane = lane_n - chunk * LANES

    def spread_map(k):
        inside = (lane >= k * p.cpc) & (lane < (k + 1) * p.cpc)
        same = row_i == chunk * p.cpc + lane - k * p.cpc
        return jnp.where(inside & same, 1.0, 0.0).astype(BF)

    for k in range(4, 7):
        loads[k].wait()
    maps = [spread_map(k) for k in range(3)]
    s_in[...] = (dot(sgv[...], maps[0], 0, 0) + dot(suv[...], maps[1], 0, 0)).astype(BF)
    s_back[...] = dot(sdv[...], maps[2], 0, 0).astype(BF)
    s_out_w[...] = (dot(maps[1], sgv[...], 0, 0) + dot(maps[2], suv[...], 0, 0)).astype(BF)

    ids = (
        ep * p.experts + lax.broadcasted_iota(jnp.int32, (p.e_rows, p.tok), 0)
    ).astype(F32)
    before = jnp.where(
        lax.broadcasted_iota(jnp.int32, (p.tok, p.tok), 0)
        < lax.broadcasted_iota(jnp.int32, (p.tok, p.tok), 1),
        1.0,
        0.0,
    ).astype(BF)
    place_in = lax.broadcasted_iota(jnp.int32, (p.slots, p.tok), 0).astype(F32)
    spare = p.rows - p.experts * p.slots

    def route(w):
        sums = [jnp.zeros((p.slots, 1), F32) for _ in range(p.experts)]
        for i in range(p.bpw):
            info = all_meta[order[w * p.bpw + i]]
            chosen = jnp.zeros((p.e_rows, p.tok), F32)
            weight_of = jnp.zeros((p.e_rows, p.tok), F32)
            for k in range(p.picks):
                same = info[k : k + 1, :] == ids
                chosen = jnp.where(same, 1.0, chosen)
                weight_of = jnp.where(
                    same, info[p.picks + k : p.picks + k + 1, :], weight_of
                )
            rank = dot(chosen.astype(BF), before, 1, 0)
            slot = jnp.where(chosen > 0.0, rank + float(p.capacity * i), -1.0)
            for e in range(p.experts):
                hot = place_in == slot[e : e + 1, :]
                oh[w, i, pl.ds(e * p.slots, p.slots), :] = jnp.where(hot, 1.0, 0.0).astype(BF)
                sums[e] = sums[e] + jnp.sum(
                    jnp.where(hot, weight_of[e : e + 1, :], 0.0), axis=1, keepdims=True
                )
            if spare:
                oh[w, i, pl.ds(p.experts * p.slots, spare), :] = jnp.zeros((spare, p.tok), BF)
        for e in range(p.experts):
            rw[w, pl.ds(e * p.slots, p.slots), :] = jnp.broadcast_to(sums[e], (p.slots, LANES))
        if spare:
            rw[w, pl.ds(p.experts * p.slots, spare), :] = jnp.zeros((spare, LANES), F32)

    def pick(w, source):
        total = dot(oh[w, 0], source[order[w * p.bpw]], 1, 0)
        for i in range(1, p.bpw):
            total = total + dot(oh[w, i], source[order[w * p.bpw + i]], 1, 0)
        return total

    def wave_rows(w, source):
        return join([source[order[w * p.bpw + i]] for i in range(p.bpw)], 0)

    def swap_copy(w):
        return remote(full.at[w, 1 - parity], got.at[w], a_s.at[w], a_r.at[w], partner)

    def put(w, e, kind, value):
        q, at = p.strip(e)
        for c in range(nc):
            full[
                w, q // nr, (q % nr) * nc + c, pl.ds(kind * p.rc + at, p.slots), :
            ] = value[:, c * LANES : (c + 1) * LANES]

    def fill(w):
        if w == 0 and p.bpw > 1:
            take_wave(0, (0, 1))
        if w > 0 or p.bpw > 1:
            route(w)
            recv_x[w] = pick(w, all_x).astype(BF)
        if w == 0:
            loads[7].wait()
            loads[8].wait()
        for kind, weight in ((0, wg), (1, wu)):
            for e in range(p.experts):
                put(w, e, kind, dot(recv_x[w, pl.ds(e * p.slots, p.slots), :], weight[e], 1, 0))
        take_wave(w, (2,))
        recv_dy = pick(w, all_dy)
        weighted[w] = (rw[w][:, :1] * recv_dy).astype(BF)
        narrow_dy = recv_dy.astype(BF)
        if w == 0:
            loads[9].wait()
        for e in range(p.experts):
            put(w, e, 2, dot(narrow_dy[e * p.slots : (e + 1) * p.slots, :], wd[e], 1, 1))
        for s in range(p.experts, p.rows // p.slots):
            for kind in range(3):
                put(w, s, kind, jnp.zeros((p.slots, p.ff), F32))
        s = dot(wave_rows(w, all_x), s_in[...], 1, 0) + dot(
            wave_rows(w, all_dy), s_back[...], 1, 0
        )
        for q in range(2 * nr):
            for c in range(nc):
                full[w, q // nr, (q % nr) * nc + c, pl.ds(3 * p.rc, p.sc), :] = s[
                    q * p.sc : (q + 1) * p.sc, c * LANES : (c + 1) * LANES
                ]
        swap_copy(w).start()

    def scatter_copy(w, d):
        return remote(
            held.at[w, others[d]], landed.at[w, d], b_s.at[w, d], b_r.at[w, d], places[d]
        )

    def scatter(w):
        swap_copy(w).wait_recv()
        for d, j in enumerate(others):
            held[w, j] = (full[w, parity, j] + got[w, j]).astype(BF)
            scatter_copy(w, d).start()

    def gather_copy(w, d, block):
        ref = acts.at[w, block, pl.ds(0, p.first)]
        return remote(ref, ref, c_s.at[w, d], c_r.at[w, d], places[d])

    def side_copy(w, d, block):
        ref = acts.at[w, block, pl.ds(0, p.first)]
        return remote(ref, ref, d_s.at[w, d], d_r.at[w, d], partner)

    def hidden_copy(d, block):
        ref = acts.at[:, block, pl.ds(p.first, p.rc)]
        return remote(ref, ref, h_s.at[d], h_r.at[d], places[d])

    def hidden_side(d, block):
        ref = acts.at[:, block, pl.ds(p.first, p.rc)]
        return remote(ref, ref, h_s.at[half + d], h_r.at[half + d], partner)

    def activate(w):
        out = full[w, parity, mine] + got[w, mine]
        for d in range(half - 1):
            scatter_copy(w, d).wait_recv()
            out = out + landed[w, d].astype(F32)
        gate, up, back = (out[k * p.rc : (k + 1) * p.rc] for k in range(3))
        silu_out, silu_slope = silu_parts(gate)
        hidden = (silu_out * up).astype(BF)
        band = parity * nr + mine // nc
        weight = rw[w, pl.ds(pl.multiple_of(band * p.rc, p.rc), p.rc), :]
        dhidden = weight * back
        acts[w, place, pl.ds(0, p.rc), :] = (dhidden * up * silu_slope).astype(BF)
        acts[w, place, pl.ds(p.rc, p.rc), :] = (dhidden * silu_out).astype(BF)
        acts[w, place, pl.ds(p.first, p.rc), :] = hidden
        dots = dot(
            jnp.ones((16, LANES), F32), hidden.astype(F32) * back, 1, 1, lax.Precision.HIGHEST
        )
        high = dots.astype(BF).astype(F32)
        mid = (dots - high).astype(BF).astype(F32)
        low = dots - high - mid
        line = lax.broadcasted_iota(jnp.int32, dots.shape, 0)
        pieces = jnp.where(line == 0, high, jnp.where(line == 1, mid, low))
        acts[w, place, pl.ds(2 * p.rc, 16), pl.ds(0, p.rc)] = pieces.astype(BF)
        both = out[3 * p.rc :]
        at = lax.broadcasted_iota(jnp.int32, both.shape, 1)
        s_up = pltpu.roll(both, LANES - p.cpc, 1)
        s_bk = pltpu.roll(both, LANES - 2 * p.cpc, 1)
        s_out, s_slope = silu_parts(both)
        s_dgate = pltpu.roll(s_bk * s_up * s_slope, p.cpc, 1)
        s_dup = pltpu.roll(s_bk * s_out, 2 * p.cpc, 1)
        value = jnp.where(
            at < p.cpc,
            s_out * s_up,
            jnp.where(at < 2 * p.cpc, s_dgate, jnp.where(at < 3 * p.cpc, s_dup, 0.0)),
        )
        acts[w, place, pl.ds(p.shared_at, p.sc), :] = value.astype(BF)
        for d in range(half - 1):
            gather_copy(w, d, place).start()
        side_copy(w, 0, place).start()

    def forward(w):
        for d in range(half - 1):
            block = parity * half + origins[d]
            gather_copy(w, d, block).wait_recv()
            side_copy(w, 1 + d, block).start()

    def strip_of(w, kind, e):
        q, at = p.strip(e)
        at = at + (p.first if kind == 0 else (kind - 1) * p.rc)
        return join([acts[w, p.place(q, c), pl.ds(at, p.slots), :] for c in range(nc)], 1)

    def shared_rows(w):
        return join(
            [
                join(
                    [
                        acts[w, p.place(q, c), pl.ds(p.shared_at, p.sc), :]
                        for c in range(nc)
                    ],
                    1,
                )
                for q in range(2 * nr)
            ],
            0,
        )

    def home_copies(b):
        return (
            remote(part.at[b], part_in.at[ep], r_s.at[b, 0], r_r.at[ep, 0], {"ep": b}),
            remote(wpart.at[b], wpart_in.at[ep], r_s.at[b, 1], r_r.at[ep, 1], {"ep": b}),
        )

    def send_home(w):
        side_copy(w, 0, (1 - parity) * half + mine).wait_recv()
        for d in range(half - 1):
            side_copy(w, 1 + d, (1 - parity) * half + origins[d]).wait_recv()
        row_grad = []
        for e in range(p.experts):
            row_grad.append(
                (
                    dot(strip_of(w, 1, e), wg[e], 1, 1) + dot(strip_of(w, 2, e), wu[e], 1, 1)
                ).astype(BF)
            )
        if spare:
            row_grad.append(jnp.zeros((spare, p.narrow), BF))
        row_grad = join(row_grad, 0)
        s_grad = dot(shared_rows(w), s_out_w[...], 1, 0)
        row_e = lax.broadcasted_iota(jnp.int32, (p.e_rows, p.rc), 0)
        row_l = lax.broadcasted_iota(jnp.int32, (p.e_rows, p.rc), 1)
        masked = []
        for q in range(2 * nr):
            line = jnp.zeros((1, p.rc), F32)
            for c in range(nc):
                pieces = acts[w, p.place(q, c), pl.ds(2 * p.rc, 16), pl.ds(0, p.rc)].astype(F32)
                line = line + (pieces[0:1] + pieces[1:2] + pieces[2:3])
            row = row_l + q * p.rc
            inside = (row >= row_e * p.slots) & (row < (row_e + 1) * p.slots)
            masked.append(jnp.where(inside, line, 0.0))
        for i in range(p.bpw):
            b = order[w * p.bpw + i]
            value = dot(oh[w, i], row_grad, 0, 0) + s_grad[i * p.tok : (i + 1) * p.tok, :]

            info = all_meta[b]
            dot_of = jnp.zeros((p.e_rows, p.tok), F32)
            for q in range(2 * nr):
                dot_of = dot_of + dot(
                    masked[q], oh[w, i, pl.ds(q * p.rc, p.rc), :].astype(F32), 1, 0,
                    lax.Precision.HIGHEST,
                )
            for k in range(p.picks):
                wpart[b, pl.ds(k, 1), :] = jnp.sum(
                    jnp.where(info[k : k + 1, :] == ids, dot_of, 0.0), axis=0, keepdims=True
                )
            if w == 0 and i == 0:
                own[...] = value
            else:
                part[b] = value.astype(BF)
                for c in home_copies(b):
                    c.start()

    wpart[...] = jnp.zeros_like(wpart)
    waves = p.waves
    if p.bpw == 1:
        route(0)
        recv_x[0] = pick(0, all_x).astype(BF)
    pl.semaphore_wait(barrier, n_ep + n_tp - 2)
    send_own()
    for step in range(waves):
        fill(step)
        scatter(step)
        if step + 1 < waves:
            take_wave(step + 1, (0, 1))
        if step >= 3:
            forward(step - 3)
        if step >= 1:
            activate(step - 1)
        if step >= 4:
            send_home(step - 4)
    late = max(0, waves - 3)
    if waves > 2:
        forward(late)
        for w in range(max(0, waves - 4), late + 1):
            send_home(w)
        late = late + 1
    activate(waves - 1)
    for d in range(half - 1):
        hidden_copy(d, place).start()
    hidden_side(0, place).start()
    for w in range(late, waves):
        forward(w)
        send_home(w)
    for d in range(half - 1):
        block = parity * half + origins[d]
        hidden_copy(d, block).wait_recv()
        hidden_side(1 + d, block).start()

    def stacked(strips):
        return join(strips, 0)

    def pile(ref, e):
        return stacked([ref[w, pl.ds(e * p.slots, p.slots), :] for w in range(waves)])

    def pile_acts(kind, e):
        return stacked([strip_of(w, kind, e) for w in range(waves)])

    ts[...] = jnp.zeros_like(ts)
    es[...] = jnp.zeros_like(es)
    so = stacked([shared_rows(w) for w in range(waves)])
    pair[0] = dot(so, stacked([wave_rows(w, all_x) for w in range(waves)]), 0, 0)
    pair[1] = dot(so, stacked([wave_rows(w, all_dy) for w in range(waves)]), 0, 0)
    for c in range(nc):
        size = min(p.cpc, p.cols - c * p.cpc)
        if size <= 0:
            continue
        to = pl.ds(c * p.cpc, size)
        sd_out[to, :] = pair[0 + 1, pl.ds(c * LANES, size), :]
        sg_out[to, :] = pair[0, pl.ds(c * LANES + p.cpc, size), :]
        su_out[to, :] = pair[0, pl.ds(c * LANES + 2 * p.cpc, size), :]
    sg, su, sd = sg_out[...], su_out[...], sd_out[...]
    es[0:1, :] = jnp.sum(sg * sg, axis=0, keepdims=True)
    es[1:2, :] = jnp.sum(su * su, axis=0, keepdims=True)
    last = []
    for d, q in enumerate(eps):
        last.append(remote(es, es_in.at[d], e_s.at[d], e_r.at[d], {"ep": q}))
        last[-1].start()
    ts[pl.ds(p.experts, 1), pl.ds(0, p.cols)] = row_squares(sd * sd)

    def gate_up(e):
        rows = pile(recv_x, e)
        gate = dot(rows, pile_acts(1, e), 0, 0)
        gate_out[e] = gate
        gate_sq[pl.ds(e, 1), :] = row_squares(gate * gate)
        up = dot(rows, pile_acts(2, e), 0, 0)
        up_out[e] = up
        up_sq[pl.ds(e, 1), :] = row_squares(up * up)

    for e in range(p.experts // 3):
        gate_up(e)
    hidden_side(0, (1 - parity) * half + mine).wait_recv()
    for d in range(half - 1):
        hidden_side(1 + d, (1 - parity) * half + origins[d]).wait_recv()
    for e in range(p.experts):
        down = dot(pile_acts(0, e), pile(weighted, e), 0, 0)
        down_out[e] = down
        ts[pl.ds(e, 1), :] = row_squares(down * down)
    for d, q in enumerate(tps):
        last.append(remote(ts, ts_in.at[d], t_s.at[d], t_r.at[d], {"tp": q}))
        last[-1].start()
    for e in range(p.experts // 3, p.experts):
        gate_up(e)

    total = own[...]
    w_total = wpart[ep]
    for b in eps:
        for ref, k in ((part_in, 0), (wpart_in, 1)):
            remote(ref.at[b], ref.at[b], r_s.at[b, k], r_r.at[b, k], {"ep": b}).wait_recv()
        total = total + part_in[b].astype(F32)
        w_total = w_total + wpart_in[b]
    token_out[...] = total.astype(BF)
    weight_out[...] = w_total[: p.picks]
    for c in last:
        c.wait_recv()
    norms = es[...]
    for d in range(n_ep - 1):
        norms = norms + es_in[d]
    sg_sq[...] = norms[0:1]
    su_sq[...] = norms[1:2]
    rows = ts[...]
    for d in range(n_tp - 1):
        rows = rows + ts_in[d]
    down_sq[...] = rows[: p.experts]
    sd_sq[...] = rows[p.experts : p.experts + 1, : p.cols]

    for cond, side, step in ((go_right, 0, 1), (go_left, 1, -1)):

        @pl.when(cond)
        def _(side=side, step=step):
            for k in range(3):
                relay(ep, k, zo.at[side, k], step).wait_send()

    for k in range(1, n_ep):
        b = order[k]

        @pl.when(((b < ep) & go_right) | ((b > ep) & go_left))
        def _(b=b):
            for a in range(3):
                relay(b, a, zs.at[b, a], 0).wait_send()

        for c in home_copies(b):
            c.wait_send()
    for w in range(waves):
        swap_copy(w).wait_send()
        for d in range(half - 1):
            scatter_copy(w, d).wait_send()
            gather_copy(w, d, place).wait_send()
        for d in range(half):
            side_copy(w, d, place).wait_send()
    for d in range(half - 1):
        hidden_copy(d, place).wait_send()
    for d in range(half):
        hidden_side(d, place).wait_send()
    for c in last:
        c.wait_send()


def copy_kernel(count, *refs):
    srcs, dsts, sem = refs[:count], refs[count : 2 * count], refs[2 * count]
    copies = [
        pltpu.make_async_copy(srcs[k], dsts[k], sem.at[k]) for k in range(count)
    ]
    for c in copies:
        c.start()
    for c in copies:
        c.wait()


def per_device(
    n_ep, n_tp,
    tokens, cotangent, routes, gate_weights,
    expert_gate, expert_up, expert_down,
    shared_gate, shared_up, shared_down,
):
    dma = pltpu.SemaphoreType.DMA
    vm = pltpu.VMEM
    tok, narrow = tokens.shape
    picks = routes.shape[1]
    experts, _, ff = expert_gate.shape
    p = Plan(n_ep, n_tp, tok, picks, narrow, experts, ff, shared_gate.shape[1])
    half, waves = p.half, p.waves
    meta_rows = up_to(2 * picks, 8)
    ts_rows = up_to(experts + 1, 8)
    wide = p.nc * LANES
    outs = [
        ((tok, narrow), BF), ((picks, tok), F32),
        ((experts, narrow, ff), F32), ((experts, narrow, ff), F32), ((experts, ff, narrow), F32),
        ((p.cols, narrow), F32), ((p.cols, narrow), F32), ((p.cols, narrow), F32),
        ((experts, narrow), F32), ((experts, narrow), F32), ((experts, ff), F32),
        ((1, narrow), F32), ((1, narrow), F32), ((1, p.cols), F32),
    ]
    out_shape = [jax.ShapeDtypeStruct(s, t) for s, t in outs]
    out_bytes = sum(
        up_to(s[-2], 8) * up_to(s[-1], LANES) * (s[0] if len(s) == 3 else 1) * jnp.dtype(t).itemsize
        for s, t in outs
    )
    grant = (VMEM_BYTES - out_bytes) // 2**18 * 2**18 - ROOM
    results = pl.pallas_call(
        functools.partial(main_kernel, p),
        out_shape=out_shape,
        in_specs=[HBM] * 10,
        out_specs=[VMEM] * len(outs),
        scratch_shapes=[
            vm(expert_gate.shape, BF), vm(expert_up.shape, BF), vm(expert_down.shape, BF),
            vm((p.cols, narrow), BF), vm((p.cols, narrow), BF), vm((p.cols, narrow), BF),
            vm((picks, tok), jnp.int32), vm((picks, tok), F32),
            vm((n_ep, tok, narrow), BF), vm((n_ep, tok, narrow), BF),
            vm((n_ep, meta_rows, tok), F32),
            vm((narrow, wide), BF), vm((narrow, wide), BF), vm((wide, narrow), BF),
            vm((waves, p.bpw, p.rows, tok), BF),
            vm((waves, p.rows, narrow), BF), vm((waves, p.rows, narrow), BF),
            vm((waves, p.rows, LANES), F32),
            vm((waves, 2, half, p.slab, LANES), F32),
            vm((waves, half, p.slab, LANES), F32),
            vm((waves, half, p.slab, LANES), BF),
            vm((waves, half - 1, p.slab, LANES), BF),
            vm((waves, n_tp, p.out_slab, LANES), BF),
            vm((2, wide, narrow), F32),
            vm((n_ep, tok, narrow), BF), vm((n_ep, tok, narrow), BF), vm((tok, narrow), F32),
            vm((n_ep, 8, tok), F32), vm((n_ep, 8, tok), F32),
            vm((ts_rows, ff), F32), vm((n_tp - 1, ts_rows, ff), F32),
            vm((8, narrow), F32), vm((n_ep - 1, 8, narrow), F32),
            dma((10,)), dma((2, 3)), dma((n_ep, 3)), dma((n_ep, 3)),
            dma((waves,)), dma((waves,)),
            dma((waves, half - 1)), dma((waves, half - 1)),
            dma((waves, half - 1)), dma((waves, half - 1)),
            dma((waves, half)), dma((waves, half)),
            dma((n_ep, 2)), dma((n_ep, 2)),
            dma((n_ep - 1,)), dma((n_ep - 1,)), dma((n_tp - 1,)), dma((n_tp - 1,)),
            dma((n_tp,)), dma((n_tp,)),
        ],
        compiler_params=pltpu.CompilerParams(
            collective_id=0, has_side_effects=True, vmem_limit_bytes=grant
        ),
    )(
        *[
            pltpu.with_memory_space_constraint(a, pltpu.HBM)
            for a in (
                tokens, cotangent, routes.T, gate_weights.T,
                expert_gate, expert_up, expert_down,
                shared_gate.T, shared_up.T, shared_down,
            )
        ]
    )
    count = len(outs)
    (
        token_grad, weight_grad, gate, up, down, sg, su, sd,
        gate_sq, up_sq, down_sq, sg_sq, su_sq, sd_sq,
    ) = pl.pallas_call(
        functools.partial(copy_kernel, count),
        out_shape=out_shape,
        in_specs=[VMEM] * count,
        out_specs=[HBM] * count,
        scratch_shapes=[dma((count,))],
        compiler_params=pltpu.CompilerParams(vmem_limit_bytes=20 * 1024 * 1024),
    )(*results)
    return (
        token_grad, weight_grad.T, gate, up, down, sg.T, su.T, sd,
        gate_sq, up_sq, down_sq, sg_sq[0], su_sq[0], sd_sq[0],
    )


def solution(mesh):
    n_ep, n_tp = mesh.shape["ep"], mesh.shape["tp"]
    return jax.shard_map(
        functools.partial(per_device, n_ep, n_tp),
        mesh=mesh,
        in_specs=(
            P("ep", "tp"),
            P("ep", "tp"),
            P("ep", None),
            P("ep", None),
            P("ep", "tp", None),
            P("ep", "tp", None),
            P("ep", None, "tp"),
            P("tp", None),
            P("tp", None),
            P(None, "tp"),
        ),
        out_specs=(
            P("ep", "tp"),
            P("ep", None),
            P("ep", "tp", None),
            P("ep", "tp", None),
            P("ep", None, "tp"),
            P("tp", "ep"),
            P("tp", "ep"),
            P("ep", "tp"),
            P("ep", "tp"),
            P("ep", "tp"),
            P("ep", None),
            P("tp"),
            P("tp"),
            P("ep"),
        ),
        check_vma=False,
    )
```
